256 devices in a mesh: grp: 2 (over y), ep: 64 (over z, x), tp: 2 (over core).
Axes of the slice: x: 4, y: 2, z: 16, core: 2. Of those that a mesh axis runs over, the one named last changes fastest.
The devices are a block of a 4x16x16 slice.
Arguments:
- tokens: bfloat16 [16384, 2048], P(('grp', 'ep')), parts along dimension 0, may hold values from -6 to 6
- in_gain: float32 [2048], replicated, may hold values from 0.1 to 1.9
- routing: int32 [16384, 4], P(('grp', 'ep')), parts along dimension 0, may hold values from 0 to 127, as said below
- gate_prob: float32 [16384, 4], P(('grp', 'ep')), parts along dimension 0, may hold values from 0.05 to 1
- w_gate: bfloat16 [128, 2048, 512], P('ep', None, 'tp'), may hold values from -0.125 to 0.125
- w_up: bfloat16 [128, 2048, 512], P('ep', None, 'tp'), may hold values from -0.125 to 0.125
- w_down: bfloat16 [128, 512, 2048], P('ep', 'tp')
- out_gain: float32 [2048], P('tp'), may hold values from 0.1 to 1.9
Outputs:
- output: bfloat16 [16384, 2048], P(('grp', 'ep'), 'tp'), parts along dimension 0
The draws below stay inside these ranges and needn't reach their ends.
There are 2 independent parts, one for each index of `grp`. The reference program is written for one: setup_inputs(seed, part) draws one part's arguments, and reference() takes and returns one part's arrays. A program takes and returns all parts, laid end to end along the dimension named above; an argument that names none is the same for every part. Nothing has to cross between parts.
Inputs may be any that keep to these rules, and one draw needn't show every extreme that they name: `routing`: each row names 4 different experts, all of one group (the same value of expert // 32). In the rows of one device no expert is named more than 8 times, and in every device's rows some expert is named exactly 8 times.
All inputs are finite; a program needn't handle non-finite values.
Results may differ from the reference program's by a relative error of at most 0.0077.
Values may be sent and summed in bfloat16 or wider, within the bound.
A program may use at most 64 MiB of HBM per device.

```python
import math
import jax
import jax.numpy as jnp
from jax import lax

D = 2048
FF = 512
GROUPS = 4
TOPK = 4
TOK_DEV = 128
EXPERTS = 128
EPG = 32
TOKENS = 8192
CAP = 8
GMAX = 64
N_EP = 64
N_TP = 2


def draw_routing(key, part):
    block_count = TOKENS // TOK_DEV
    key_order, key_pick, key_perm, key_shuffle = jax.random.split(key, 4)
    hot_count = min(GMAX, TOK_DEV)
    hot_span = hot_count * TOPK // CAP
    group_order = jax.random.permutation(key_order, GROUPS)
    hot_picks = jnp.minimum(jax.random.randint(key_pick, (block_count,), 0, GROUPS + 2), GROUPS - 1)
    hot_group = group_order[hot_picks]
    position = jnp.arange(TOK_DEV, dtype=jnp.int32)
    is_hot = position < hot_count
    cold_index = position - hot_count
    groups = jnp.where(is_hot[None, :], hot_group[:, None], (hot_group[:, None] + 1 + cold_index[None, :] % (GROUPS - 1)) % GROUPS)
    group_rank = jnp.where(is_hot, position, cold_index // (GROUPS - 1))
    modulus = jnp.where(is_hot, hot_span, EPG)
    within = (group_rank[:, None] * TOPK + jnp.arange(TOPK, dtype=jnp.int32)[None, :]) % modulus[:, None]
    perm_keys = jax.random.split(key_perm, block_count * GROUPS)
    orders = jax.vmap(lambda one_key: jax.random.permutation(one_key, EPG))(perm_keys).reshape(block_count, GROUPS, EPG)
    block_ids = jnp.arange(block_count)[:, None, None]
    local_ids = orders[block_ids, groups[:, :, None], within[None, :, :]]
    experts = groups[:, :, None] * EPG + local_ids
    shuffle_keys = jax.random.split(key_shuffle, block_count)
    shuffles = jax.vmap(lambda one_key: jax.random.permutation(one_key, TOK_DEV))(shuffle_keys)
    experts = jnp.take_along_axis(experts, shuffles[:, :, None], axis=1)
    return experts.reshape(TOKENS, TOPK).astype(jnp.int32)


def draw_w_down(key, part):
    key_base, key_col = jax.random.split(key)
    columns = jnp.arange(D, dtype=jnp.float32) / D
    entries_base = jax.random.normal(key_base, (EXPERTS, FF, D), jnp.float32)
    spread = jax.random.uniform(key_col, (D,), jnp.float32, 0.5, 1.5)
    col_rise = 3.0 ** columns
    return (entries_base * FF ** (-0.5) * col_rise * spread).astype(jnp.bfloat16)


def levels(own_key, dims, cuts, low, largest):
    def one(dim, parts):
        draws = jax.random.uniform(jax.random.fold_in(jax.random.fold_in(own_key, 6), dim), (parts,), jnp.float32, low / len(cuts), largest / len(cuts))
        return jnp.repeat(jnp.exp(draws), dims[dim] // parts).reshape((-1,) + (1,) * (len(dims) - dim - 1))

    gain = one(*cuts[0])
    for cut in cuts[1:]:
        gain = gain * one(*cut)
    return gain


def bell_draw(rng, extent, width, most, cuts=(), kind=jnp.bfloat16):
    result = jax.random.normal(rng, extent, jnp.float32) * width
    if len(cuts) > 0:
        result = levels(rng, extent, cuts, -0.22, 0.18) * result
    return jnp.clip(result, min=-most, max=most).astype(kind)


def setup_inputs(seed: int = 0, part: int = 0) -> dict:
    seeds = jax.random.split(jax.random.key(seed), 9)
    part_keys = jax.random.split(jax.random.fold_in(seeds[8], part), 9)
    tokens = bell_draw(part_keys[0], (TOKENS, D), 1.0, 6.0, ((0, 64),))
    in_gain = jnp.clip(1.0 + 0.18 * jax.random.normal(seeds[1], (D,), jnp.float32), 0.1, 1.9)
    routing = draw_routing(jax.random.fold_in(jax.random.fold_in(seeds[8], part), 71), part)
    gate_prob = jnp.clip(jnp.exp(math.log(1.0) - 2.9957323 * jax.random.uniform(part_keys[3], (TOKENS, TOPK), jnp.float32) ** levels(part_keys[3], (TOKENS, TOPK), ((0, 64),), -0.2, 0.2)), 0.05, 1.0)
    w_gate = bell_draw(seeds[4], (EXPERTS, D, FF), D ** -0.5, 0.125, ((0, 64), (2, 2)))
    w_up = bell_draw(seeds[5], (EXPERTS, D, FF), D ** -0.5, 0.125, ((0, 64), (2, 2)))
    w_down = draw_w_down(jax.random.fold_in(seeds[8], 71), part)
    out_gain = jnp.clip(1.0 + 0.18 * jax.random.normal(seeds[7], (D,), jnp.float32), 0.1, 1.9)
    return dict(tokens=tokens, in_gain=in_gain, routing=routing, gate_prob=gate_prob, w_gate=w_gate, w_up=w_up, w_down=w_down, out_gain=out_gain)


EPS = 1e-06

def slot_ranks(flat_routes):
    matches = (flat_routes[:, None] == jnp.arange(EXPERTS, dtype=jnp.int32)[None, :]).astype(jnp.int32)
    earlier = jnp.cumsum(matches, axis=0) - matches
    return lax.optimization_barrier(jnp.sum(earlier * matches, axis=1)).astype(jnp.int32)

def reference(tokens, in_gain, routing, gate_prob, w_gate, w_up, w_down, out_gain):
    floats = tokens.astype(jnp.float32)
    normed = (floats * lax.rsqrt(lax.optimization_barrier(jnp.mean(floats * floats, axis=-1, keepdims=True)) + EPS) * in_gain).astype(jnp.bfloat16)
    blocks = routing.reshape(N_EP, TOK_DEV * TOPK)
    slot_rank = jax.vmap(slot_ranks)(blocks)
    sources = jnp.arange(N_EP, dtype=jnp.int32)[:, None]
    slot_ids = (blocks * (N_EP * CAP) + sources * CAP + slot_rank).reshape(-1).astype(jnp.int32)
    token_ids = jnp.arange(TOKENS * TOPK, dtype=jnp.int32) // TOPK
    slot_table = jnp.zeros((EXPERTS * N_EP * CAP,), jnp.int32).at[slot_ids].set(token_ids + 1)
    slot_table = slot_table.reshape(EXPERTS, N_EP * CAP)

    def expert(inputs):
        entries, gate_w, up_w, down_w = inputs
        filled = entries > 0
        rows_in = jnp.where(filled[:, None], normed[jnp.maximum(entries - 1, 0)], jnp.zeros((), jnp.bfloat16))
        gate_act = jnp.dot(rows_in, gate_w, preferred_element_type=jnp.float32)
        up_act = jnp.dot(rows_in, up_w, preferred_element_type=jnp.float32)
        hidden = (jax.nn.silu(gate_act) * up_act).astype(jnp.bfloat16)
        pieces = jnp.einsum('rnf,nfd->nrd', hidden.reshape(-1, N_TP, FF // N_TP).astype(jnp.float32), down_w.reshape(N_TP, FF // N_TP, D).astype(jnp.float32))
        rounded = lax.optimization_barrier(pieces.astype(jnp.bfloat16))
        return lax.optimization_barrier(jnp.sum(rounded.astype(jnp.float32), axis=0)).astype(jnp.bfloat16)
    results = lax.map(expert, (slot_table, w_gate, w_up, w_down))
    picked = results.reshape(-1, D)[slot_ids].astype(jnp.float32).reshape(TOKENS, TOPK, D)
    mixed_rows = lax.optimization_barrier(jnp.sum(picked * gate_prob[:, :, None], axis=1))
    inv_rms = lax.rsqrt(lax.optimization_barrier(jnp.mean(mixed_rows * mixed_rows, axis=-1, keepdims=True)) + EPS)
    return (mixed_rows * inv_rms * out_gain).astype(jnp.bfloat16)
```

```python
import functools
import math

import jax
import jax.numpy as jnp
from jax import lax
from jax.experimental import pallas as pl
from jax.experimental.pallas import tpu as pltpu
from jax.sharding import PartitionSpec as P

GROUPS = 4
EPS = 1e-06
MESH = pl.DeviceIdType.MESH
F32 = jnp.float32
BF16 = jnp.bfloat16
I32 = jnp.int32


def iota(shape, dim):
    return lax.broadcasted_iota(I32, shape, dim)


def mm(a, b):
    return jnp.dot(a, b, preferred_element_type=F32)


def mm_tn(a, b):
    return lax.dot_general(a, b, (((0,), (0,)), ((), ())), preferred_element_type=F32)


def kernel(
    cfg, routing, prob, tokens, gain, out_gain, wg_hbm, wu_hbm, wd_hbm, out_ref,
    wg, wu, wd, place, meta_out, meta_in, packed, zbuf, mix_hi, mix_lo, xsend, rows, hid,
    back_out, back_in, part, psend, rz, side, ret, own_part, sq_out, sq_in,
    w_sem, wd_send, wd_recv, m_send, m_recv, i_send, z_send, z_recv, x_send, x_recv,
    d_send, d_recv, h_send, h_recv, b_send, b_recv, p_send, c_recv, side_recv, ret_recv,
    q_send, q_recv,
):
    lines, side_len, tok, top, cap, gmax, half, width, epg = cfg
    cols, deep = side_len, side_len
    me = lax.axis_index("ep")
    core = lax.axis_index("tp")
    peer = 1 - core
    x, z = lax.rem(me, cols), lax.div(me, cols)
    grp, o = lax.div(z, deep), lax.rem(z, deep)
    late = lax.div(o, deep // 2)
    loc = wg.shape[0]

    def at_z(zz):
        return {"ep": zz * cols + x}

    def at_x(xx):
        return {"ep": z * cols + xx}

    def remote(src, dst, s, r, dev):
        return pltpu.make_async_remote_copy(
            src_ref=src, dst_ref=dst, send_sem=s, recv_sem=r, device_id=dev, device_id_type=MESH
        )

    other_core = {"tp": peer}
    my_cols = pl.ds(pl.multiple_of(core * half, half), half)
    peer_cols = pl.ds(pl.multiple_of(peer * half, half), half)

    barrier = pltpu.get_barrier_semaphore()
    for j in range(1, lines):
        pl.semaphore_signal(barrier, 1, device_id=at_z(lax.rem(z + j, lines)), device_id_type=MESH)
    for j in range(1, cols):
        pl.semaphore_signal(barrier, 1, device_id=at_x(lax.rem(x + j, cols)), device_id_type=MESH)
    pl.semaphore_signal(barrier, 1, device_id=other_core, device_id_type=MESH)

    w_copies = [
        pltpu.make_async_copy(wg_hbm, wg, w_sem.at[0]),
        pltpu.make_async_copy(wu_hbm, wu, w_sem.at[1]),
        pltpu.make_async_copy(wd_hbm.at[:, :, my_cols], wd.at[core], w_sem.at[2]),
    ]
    for copy in w_copies:
        copy.start()

    r_k = [routing[k : k + 1, :] for k in range(top)]
    g_t = lax.div(r_k[0], epg)
    experts = epg * GROUPS
    earlier = (iota((tok, tok), 0) < iota((tok, tok), 1)).astype(BF16)
    e_io = iota((experts, tok), 0)
    named = jnp.zeros((experts, tok), F32)
    for k in range(top):
        named = named + (e_io == r_k[k]).astype(F32)
    rank = mm(named.astype(BF16), earlier)
    g_io = iota((16, tok), 0)
    in_group = (g_io == g_t).astype(F32)
    g_rank = mm(in_group.astype(BF16), earlier)
    pos = jnp.sum(in_group * g_rank, axis=0, keepdims=True).astype(I32)
    for k in range(top):
        rank_k = jnp.sum(jnp.where(e_io == r_k[k], rank, 0.0), axis=0, keepdims=True)
        sq_out[k : k + 1, :] = ((r_k[k] - g_t * epg) * cap + 1).astype(F32) + rank_k
        sq_out[top + k : top + k + 1, :] = prob[k : k + 1, :]
    wide = 2 * gmax
    wr = iota((GROUPS * wide, tok), 0)
    sel2 = (wr == g_t * wide + pos) | (wr == g_t * wide + gmax + pos)
    meta = lax.dot_general(
        sq_out[0 : 2 * top, :], sel2.astype(F32), (((1,), (1,)), ((), ())),
        preferred_element_type=F32, precision=lax.Precision.HIGHEST,
    )
    for g in range(GROUPS):
        meta_out[g] = meta[:, g * wide : (g + 1) * wide]
    place[...] = (iota((GROUPS * gmax, tok), 0) == g_t * gmax + pos).astype(BF16)

    floats = tokens[...].astype(F32)
    inv = lax.rsqrt(jnp.mean(floats * floats, axis=-1, keepdims=True) + EPS)
    normed = (tokens[:, my_cols].astype(F32) * inv * gain[:, my_cols]).astype(BF16)
    packed[...] = mm(place[...], normed).astype(BF16).reshape(packed.shape)

    pl.semaphore_wait(barrier, (lines - 1) + (cols - 1) + 1)

    def rel(a):
        return lax.rem(a + 2 * GROUPS, GROUPS)

    def meta_copy(j):
        zt = lax.rem(z + j, lines)
        gt = lax.div(zt, deep)
        return remote(
            meta_out.at[gt], meta_in.at[rel(grp - gt), o], m_send.at[j], m_recv.at[j], at_z(zt)
        )

    for j in range(1, lines):
        meta_copy(j).start()

    def first(t, row):
        gt = lax.rem(grp + t, GROUPS)
        d = (GROUPS - t) % GROUPS
        return remote(
            packed.at[gt], zbuf.at[d, o], i_send.at[t], z_recv.at[d, o], at_z(gt * deep + row)
        )

    opp = first(2, (deep - 1) * (1 - late))
    nxt = first(1, 0)
    prv = first(3, deep - 1)
    own_up = remote(packed.at[grp], zbuf.at[0, o], i_send.at[0], z_recv.at[0, o], at_z(lax.rem(z + 1, lines)))
    own_dn = remote(packed.at[grp], zbuf.at[0, o], i_send.at[4], z_recv.at[0, o], at_z(lax.rem(z + lines - 1, lines)))
    opp.start()
    nxt.start()
    prv.start()
    pl.when(o < deep - 1)(own_up.start)
    pl.when(o > 0)(own_dn.start)
    wd_copy = remote(wd_hbm.at[:, :, peer_cols], wd.at[core], wd_send.at[0], wd_recv.at[0], other_core)
    wd_copy.start()
    zbuf[0, o] = packed[grp]
    meta_in[0, o] = meta_out[grp]

    def onward(plus):
        zz = lax.rem(z + plus * 2 - 1 + lines, lines)
        more = ((plus == 1) & (o < deep - 1)) | ((plus == 0) & (o > 0))
        return zz, more

    def z_copy(d, s, plus):
        zz, more = onward(plus)
        return remote(zbuf.at[d, s], zbuf.at[d, s], z_send.at[d, s], z_recv.at[d, s], at_z(zz)), more

    def arrive(d, s, plus):
        copy, more = z_copy(d, s, plus)
        copy.wait_recv()
        pl.when(more)(copy.start)

    d_near, d_far = 3 - 2 * late, 1 + 2 * late
    plus_near, plus_far = 1 - late, late
    half_deep = deep // 2

    def opp_item(j):
        s = lax.rem(j + half_deep * (1 - late), deep)
        return s, lax.div(s, half_deep)

    def own_item(j):
        s = lax.rem(o + j, deep)
        return s, (s < o).astype(I32)

    def arrive_opp(js):
        for j in js:
            s, plus = opp_item(j)
            arrive(2, s, plus)

    def arrive_side(d, plus):
        for s in range(deep):
            arrive(d, s, plus)

    def arrive_own():
        for j in range(1, deep):
            s, plus = own_item(j)
            arrive(0, s, plus)

    quad = deep * gmax
    piece = loc * deep * cap

    def x_copy(d, j):
        xx = lax.rem(x + j, cols)
        return remote(xsend.at[d, xx], rows.at[core, d, x], x_send.at[d, j], x_recv.at[d, j], at_x(xx))

    def x_arrival(d, j):
        xx = lax.rem(x + cols - j, cols)
        return remote(xsend.at[d, xx], rows.at[core, d, xx], x_send.at[d, j], x_recv.at[d, j], at_x(xx))

    def d_copy(d, j):
        xx = lax.rem(x + cols - j, cols)
        return remote(rows.at[core, d, xx], rows.at[core, d, xx], d_send.at[d, j], d_recv.at[d, j], other_core)

    def d_arrival(d, j):
        xx = lax.rem(x + cols - j, cols)
        return remote(rows.at[peer, d, xx], rows.at[peer, d, xx], d_send.at[d, j], d_recv.at[d, j], other_core)

    def select(d):
        lane = iota((2 * top, wide), 1)
        pairs = [
            jnp.where(lane < gmax, meta_in[d, 2 * i], meta_in[d, 2 * i + 1]) for i in range(deep // 2)
        ]
        info = jnp.concatenate(pairs, axis=1)
        zs = lax.div(iota((1, quad), 1), gmax)
        s_io = iota((quad, quad), 0)
        a = jnp.zeros((quad, quad), F32)
        w = jnp.zeros((quad, quad), F32)
        span = cols * loc * cap
        for k in range(top):
            v = info[k : k + 1, :].astype(I32) - 1 - span * o
            ok = (v >= 0) & (v < span)
            sid = jnp.where(ok, lax.div(v, cap) * (deep * cap) + zs * cap + lax.rem(v, cap), -1)
            hit = s_io == sid
            a = jnp.where(hit, 1.0, a)
            w = jnp.where(hit, info[top + k : top + k + 1, :], w)
        hi = w.astype(BF16)
        mix_hi[d] = hi
        mix_lo[d] = (w - hi.astype(F32)).astype(BF16)
        picked = mm(a.astype(BF16), zbuf[d].reshape(quad, half)).astype(BF16)
        xsend[d] = picked.reshape(cols, piece, half)
        for j in range(1, cols):
            x_copy(d, j).start()
        rows[core, d, x] = xsend[d, x]
        d_copy(d, 0).start()

    def exchange(d):
        for j in range(1, cols):
            x_arrival(d, j).wait_recv()
            d_copy(d, j).start()

    m = cols * deep * cap
    ff = wg.shape[2]

    def h_copy(d):
        return remote(hid.at[core, d], hid.at[core, d], h_send.at[d], h_recv.at[d], other_core)

    def h_arrival(d):
        return remote(hid.at[peer, d], hid.at[peer, d], h_send.at[d], h_recv.at[d], other_core)

    def gate_up(d):
        for j in range(cols):
            d_arrival(d, j).wait_recv()
        for e in range(loc):
            r = [
                rows[h, d, :, e * deep * cap : (e + 1) * deep * cap, :].reshape(m, half) for h in range(2)
            ]
            ga = mm(r[0], wg[e, :half, :]) + mm(r[1], wg[e, half:, :])
            up = mm(r[0], wu[e, :half, :]) + mm(r[1], wu[e, half:, :])
            hid[core, d, e] = (ga / (1.0 + jnp.exp(-ga)) * up).astype(BF16)
        h_copy(d).start()

    def b_copy(d, j):
        xx = lax.rem(x + j, cols)
        return remote(back_out.at[d, xx], back_in.at[d, x], b_send.at[d, j], b_recv.at[d, j], at_x(xx))

    def b_arrival(d, j):
        xx = lax.rem(x + cols - j, cols)
        return remote(back_out.at[d, xx], back_in.at[d, xx], b_send.at[d, j], b_recv.at[d, j], at_x(xx))

    def down(d):
        h_arrival(d).wait_recv()
        for e in range(loc):
            y = mm(hid[0, d, e], wd[0, e]) + mm(hid[1, d, e], wd[1, e])
            back_out[d, :, e * deep * cap : (e + 1) * deep * cap, :] = y.astype(BF16).reshape(
                cols, deep * cap, half
            )
        for j in range(1, cols):
            b_copy(d, j).start()
        back_in[d, x] = back_out[d, x]

    def home_copy(d, s, plus):
        direct = jnp.where(plus == 1, 0, deep - 1)
        gs = lax.rem(grp + d, GROUPS)
        return remote(
            psend.at[d, s], ret.at[grp], p_send.at[d, s], ret_recv.at[lax.rem(GROUPS - d, GROUPS)],
            at_z(gs * deep + s),
        ), o == direct

    def chain_copy(d, s, plus):
        zz = lax.rem(z - (plus * 2 - 1) + lines, lines)
        return remote(psend.at[d, s], rz.at[d, s], p_send.at[d, s], c_recv.at[d, s], at_z(zz))

    def side_copy(s, plus):
        zz = lax.rem(z - (plus * 2 - 1) + lines, lines)
        return remote(psend.at[0, s], side.at[1 - plus], p_send.at[0, s], side_recv.at[1 - plus], at_z(zz))

    def add_up(d, s, plus):
        _, more = onward(plus)
        mine = pl.ds(s * gmax, gmax)

        @pl.when(more)
        def _():
            chain_copy(d, s, plus).wait_recv()
            psend[d, s] = (part[mine, :] + rz[d, s].astype(F32)).astype(BF16)

        @pl.when(jnp.logical_not(more))
        def _():
            psend[d, s] = part[mine, :].astype(BF16)

    def combine(d):
        for j in range(1, cols):
            b_arrival(d, j).wait_recv()
        res = back_in[d].reshape(quad, half)
        part[...] = mm_tn(mix_hi[d], res) + mm_tn(mix_lo[d], res)

    def send_far(d, s, plus):
        add_up(d, s, plus)
        home, last = home_copy(d, s, plus)
        pl.when(last)(home.start)
        pl.when(jnp.logical_not(last))(chain_copy(d, s, plus).start)

    def far_opp(j):
        s = lax.rem(j + half_deep * late, deep)
        return s, lax.div(s, half_deep)

    def combine_opp():
        combine(2)
        for j in range(deep):
            s, plus = far_opp(j)
            send_far(2, s, plus)

    def combine_side(d, plus):
        combine(d)
        for s in range(deep):
            send_far(d, s, plus)

    def own_order(j):
        s = late * j + (1 - late) * (deep - 1 - j)
        return s, (s < o).astype(I32)

    def combine_own():
        combine(0)
        for j in range(deep):
            s, plus = own_order(j)

            @pl.when(s == o)
            def _():
                own_part[...] = part[pl.ds(s * gmax, gmax), :]

            @pl.when(s != o)
            def _():
                add_up(0, s, plus)
                near = s + plus * 2 - 1 == o
                pl.when(near)(side_copy(s, plus).start)
                pl.when(jnp.logical_not(near))(chain_copy(0, s, plus).start)

    arrive_opp(range(deep))
    for j in range(1, lines):
        meta_copy(j).wait_recv()
    select(2)
    arrive_side(d_near, plus_near)
    select(d_near)
    exchange(2)
    w_copies[0].wait()
    w_copies[1].wait()
    gate_up(2)
    arrive_side(d_far, plus_far)
    select(d_far)
    exchange(d_near)
    w_copies[2].wait()
    wd_arrival = remote(wd_hbm.at[:, :, my_cols], wd.at[peer], wd_send.at[0], wd_recv.at[0], other_core)
    wd_arrival.wait_recv()
    down(2)
    gate_up(d_near)
    arrive_own()
    select(0)
    exchange(d_far)
    down(d_near)
    gate_up(d_far)
    exchange(0)
    down(d_far)
    combine_opp()
    gate_up(0)
    combine_side(d_far, plus_far)
    down(0)
    combine_side(d_near, plus_near)
    combine_own()

    for t in range(1, GROUPS):
        gt = lax.rem(grp + t, GROUPS)
        remote(psend.at[t, o], ret.at[gt], p_send.at[t, o], ret_recv.at[t], at_z(z)).wait_recv()

    @pl.when(o < deep - 1)
    def _():
        side_copy(o, 1).wait_recv()
        own_part[...] += side[0].astype(F32)

    @pl.when(o > 0)
    def _():
        side_copy(o, 0).wait_recv()
        own_part[...] += side[1].astype(F32)

    ret[grp] = own_part[...].astype(BF16)
    mixed = mm_tn(place[...], ret[...].reshape(GROUPS * gmax, half))
    sq = jnp.zeros((tok, 128), F32)
    for i in range(half // 128):
        v = mixed[:, i * 128 : (i + 1) * 128]
        sq = sq + v * v
    sq_out[...] = sq
    q_copy = remote(sq_out, sq_in, q_send.at[0], q_recv.at[0], other_core)
    q_copy.start()
    q_copy.wait_recv()
    total = jnp.sum(sq_out[...] + sq_in[...], axis=1, keepdims=True)
    out_ref[...] = (mixed * lax.rsqrt(total / width + EPS) * out_gain[...]).astype(BF16)

    q_copy.wait_send()
    for j in range(1, lines):
        meta_copy(j).wait_send()
    opp.wait_send()
    nxt.wait_send()
    prv.wait_send()
    pl.when(o < deep - 1)(own_up.wait_send)
    pl.when(o > 0)(own_dn.wait_send)
    wd_copy.wait_send()

    def sent(d, s, plus):
        copy, more = z_copy(d, s, plus)
        pl.when(more)(copy.wait_send)
        chain_copy(d, s, plus).wait_send()

    for s in range(deep):
        sent(2, s, s // half_deep)
        sent(3, s, 1)
        sent(1, s, 0)
    for j in range(1, deep):
        s, plus = own_item(j)
        sent(0, s, plus)
    for d in range(GROUPS):
        h_copy(d).wait_send()
        d_copy(d, 0).wait_send()
        for j in range(1, cols):
            d_copy(d, j).wait_send()
            x_copy(d, j).wait_send()
            b_copy(d, j).wait_send()


def body(tokens, in_gain, routing, gate_prob, w_gate, w_up, w_down, out_gain):
    ep_count = lax.axis_size("ep")
    loc, width, ff = w_gate.shape
    tok, top = routing.shape
    half = out_gain.shape[0]
    epg = loc * ep_count // GROUPS
    cap = max(2, tok * top // (2 * epg))
    gmax = epg * cap // top
    side = math.isqrt(ep_count // GROUPS)
    lines = ep_count // side
    cols, deep = side, side
    quad = deep * gmax
    piece = loc * deep * cap
    m = cols * deep * cap
    cfg = (lines, side, tok, top, cap, gmax, half, width, epg)
    vmem = pl.BlockSpec(memory_space=pltpu.VMEM)
    anyw = pl.BlockSpec(memory_space=pl.ANY)
    dma = pltpu.SemaphoreType.DMA
    scratch = [
        pltpu.VMEM(w_gate.shape, BF16),
        pltpu.VMEM(w_up.shape, BF16),
        pltpu.VMEM((2, loc, ff, half), BF16),
        pltpu.VMEM((GROUPS * gmax, tok), BF16),
        pltpu.VMEM((GROUPS, 2 * top, 2 * gmax), F32),
        pltpu.VMEM((GROUPS, deep, 2 * top, 2 * gmax), F32),
        pltpu.VMEM((GROUPS, gmax, half), BF16),
        pltpu.VMEM((GROUPS, deep, gmax, half), BF16),
        pltpu.VMEM((GROUPS, quad, quad), BF16),
        pltpu.VMEM((GROUPS, quad, quad), BF16),
        pltpu.VMEM((GROUPS, cols, piece, half), BF16),
        pltpu.VMEM((2, GROUPS, cols, piece, half), BF16),
        pltpu.VMEM((2, GROUPS, loc, m, ff), BF16),
        pltpu.VMEM((GROUPS, cols, piece, half), BF16),
        pltpu.VMEM((GROUPS, cols, piece, half), BF16),
        pltpu.VMEM((quad, half), F32),
        pltpu.VMEM((GROUPS, deep, gmax, half), BF16),
        pltpu.VMEM((GROUPS, deep, gmax, half), BF16),
        pltpu.VMEM((2, gmax, half), BF16),
        pltpu.VMEM((GROUPS, gmax, half), BF16),
        pltpu.VMEM((gmax, half), F32),
        pltpu.VMEM((tok, 128), F32),
        pltpu.VMEM((tok, 128), F32),
        dma((3,)),
        dma((1,)),
        dma((1,)),
        dma((lines,)),
        dma((lines,)),
        dma((5,)),
        dma((GROUPS, deep)),
        dma((GROUPS, deep)),
        dma((GROUPS, cols)),
        dma((GROUPS, cols)),
        dma((GROUPS, cols)),
        dma((GROUPS, cols)),
        dma((GROUPS,)),
        dma((GROUPS,)),
        dma((GROUPS, cols)),
        dma((GROUPS, cols)),
        dma((GROUPS, deep)),
        dma((GROUPS, deep)),
        dma((2,)),
        dma((GROUPS,)),
        dma((1,)),
        dma((1,)),
    ]
    return pl.pallas_call(
        functools.partial(kernel, cfg),
        out_shape=jax.ShapeDtypeStruct((tok, half), BF16),
        in_specs=[vmem] * 5 + [anyw] * 3,
        out_specs=vmem,
        scratch_shapes=scratch,
        compiler_params=pltpu.CompilerParams(
            collective_id=0, has_side_effects=True, vmem_limit_bytes=60 * 1024 * 1024
        ),
    )(
        routing.T, gate_prob.T, tokens, in_gain.reshape(1, width), out_gain.reshape(1, half),
        w_gate, w_up, w_down,
    )


def solution(mesh):
    placed = (
        P(("grp", "ep"), None),
        P(),
        P(("grp", "ep"), None),
        P(("grp", "ep"), None),
        P("ep", None, "tp"),
        P("ep", None, "tp"),
        P("ep", "tp", None),
        P("tp"),
    )
    return jax.shard_map(
        body, mesh=mesh, in_specs=placed, out_specs=P(("grp", "ep"), "tp"), check_vma=False
    )
```

```python
import functools
import math

import jax
import jax.numpy as jnp
from jax import lax
from jax.experimental import pallas as pl
from jax.experimental.pallas import tpu as pltpu
from jax.sharding import PartitionSpec as P

GROUPS = 4
EPS = 1e-06
MESH = pl.DeviceIdType.MESH
F32 = jnp.float32
BF16 = jnp.bfloat16
I32 = jnp.int32


def iota(shape, dim):
    return lax.broadcasted_iota(I32, shape, dim)


def mm(a, b):
    return jnp.dot(a, b, preferred_element_type=F32)


def mm_tn(a, b):
    return lax.dot_general(a, b, (((0,), (0,)), ((), ())), preferred_element_type=F32)


ARRIVE, BACK, SELECT, EXCHANGE, GATE_UP, DOWN, COMBINE, SEND_OPP, WAIT_META, WAIT_W = range(10)

PLAN = (
    (ARRIVE, 0, 1, 0, 2), (ARRIVE, 3, 3, 0, 0), (WAIT_META, 0, 0, 0, 0), (SELECT, 0, 0, 0, 0),
    (EXCHANGE, 0, 0, 0, 0), (WAIT_W, 0, 0, 0, 0), (GATE_UP, 0, 0, 0, 0), (DOWN, 0, 0, 0, 0),
    (ARRIVE, 3, 2, 3, 3), (ARRIVE, 3, 1, 0, 3), (SELECT, 3, 1, 0, 1), (SEND_OPP, 0, 0, 0, 0),
    (ARRIVE, 3, 0, 3, 2), (SELECT, 3, 0, 3, 1), (COMBINE, 0, 0, 0, 0), (EXCHANGE, 3, 1, 0, 1),
    (GATE_UP, 3, 1, 0, 1), (DOWN, 3, 1, 0, 1), (ARRIVE, 0, 2, 3, 1), (ARRIVE, 0, 3, 1, 0),
    (EXCHANGE, 3, 0, 3, 1), (GATE_UP, 3, 0, 3, 1), (DOWN, 3, 0, 3, 1), (ARRIVE, 2, 3, 1, 1),
    (SELECT, 0, 1, 1, 0), (COMBINE, 3, 1, 0, 1), (ARRIVE, 1, 0, 3, 0), (ARRIVE, 2, 2, 1, 2),
    (SELECT, 2, 1, 3, 0), (COMBINE, 3, 0, 3, 1), (ARRIVE, 1, 1, 1, 3), (ARRIVE, 1, 2, 2, 3),
    (EXCHANGE, 0, 1, 1, 0), (SELECT, 1, 0, 1, 1), (ARRIVE, 1, 3, 2, 2), (SELECT, 1, 1, 2, 1),
    (GATE_UP, 0, 1, 1, 0), (ARRIVE, 2, 0, 2, 0), (EXCHANGE, 2, 1, 3, 0), (DOWN, 0, 1, 1, 0),
    (ARRIVE, 2, 1, 2, 1), (SELECT, 2, 0, 2, 0), (EXCHANGE, 1, 0, 1, 1), (GATE_UP, 1, 0, 3, 0),
    (EXCHANGE, 1, 1, 2, 1), (GATE_UP, 2, 1, 1, 1), (DOWN, 2, 1, 3, 0), (BACK, 0, 1, 0, 2),
    (DOWN, 1, 0, 1, 1), (GATE_UP, 1, 1, 2, 1), (COMBINE, 0, 1, 1, 0), (BACK, 0, 2, 0, 3),
    (BACK, 0, 3, 0, 0), (DOWN, 1, 1, 2, 1), (EXCHANGE, 2, 0, 2, 0), (COMBINE, 1, 0, 1, 1),
    (BACK, 1, 1, 1, 1), (GATE_UP, 2, 0, 2, 0), (BACK, 1, 0, 1, 0), (DOWN, 2, 0, 2, 0),
    (COMBINE, 2, 1, 2, 1), (COMBINE, 1, 1, 3, 0), (BACK, 1, 3, 3, 2), (BACK, 1, 2, 1, 3),
    (COMBINE, 2, 0, 2, 0), (BACK, 2, 0, 3, 3), (BACK, 2, 1, 1, 2), (BACK, 3, 2, 3, 0),
    (BACK, 3, 3, 2, 0), (BACK, 3, 0, 3, 1), (BACK, 3, 1, 2, 1), (BACK, 2, 2, 2, 2),
    (BACK, 2, 3, 2, 3),
)


def kernel(
    cfg, routing, prob, tokens, gain, out_gain, wg_hbm, wu_hbm, wd_hbm, out_ref,
    wg, wu, wd, place, meta_out, meta_in, packed, zbuf, mix_hi, mix_lo, xsend, rows, hid,
    back_out, back_in, part, psend, rz, side, ret, sq_out, sq_in,
    w_sem, wd_send, wd_recv, m_send, m_recv, i_send, z_send, z_recv, x_send, x_recv,
    d_send, d_recv, h_send, h_recv, b_send, b_recv, p_send, c_recv, side_recv, ret_recv,
    q_send, q_recv,
):
    lines, side_len, tok, top, cap, gmax, half, width, epg = cfg
    cols, deep = side_len, side_len
    two = deep // 2
    me = lax.axis_index("ep")
    core = lax.axis_index("tp")
    peer = 1 - core
    x, z = lax.rem(me, cols), lax.div(me, cols)
    grp, o = lax.div(z, deep), lax.rem(z, deep)
    late = lax.div(o, two)
    in_row = [(o == r).astype(I32) for r in range(deep)]
    loc = wg.shape[0]

    def at_z(zz):
        return {"ep": zz * cols + x}

    def at_x(xx):
        return {"ep": z * cols + xx}

    def remote(src, dst, s, r, dev):
        return pltpu.make_async_remote_copy(
            src_ref=src, dst_ref=dst, send_sem=s, recv_sem=r, device_id=dev, device_id_type=MESH
        )

    other_core = {"tp": peer}
    my_cols = pl.ds(pl.multiple_of(core * half, half), half)
    peer_cols = pl.ds(pl.multiple_of(peer * half, half), half)

    barrier = pltpu.get_barrier_semaphore()
    for j in range(1, lines):
        pl.semaphore_signal(barrier, 1, device_id=at_z(lax.rem(z + j, lines)), device_id_type=MESH)
    for j in range(1, cols):
        pl.semaphore_signal(barrier, 1, device_id=at_x(lax.rem(x + j, cols)), device_id_type=MESH)
    pl.semaphore_signal(barrier, 1, device_id=other_core, device_id_type=MESH)

    w_copies = [
        pltpu.make_async_copy(wg_hbm, wg, w_sem.at[0]),
        pltpu.make_async_copy(wu_hbm, wu, w_sem.at[1]),
        pltpu.make_async_copy(wd_hbm.at[:, :, my_cols], wd.at[core], w_sem.at[2]),
    ]
    for copy in w_copies:
        copy.start()

    r_k = [routing[k : k + 1, :] for k in range(top)]
    g_t = lax.div(r_k[0], epg)
    experts = epg * GROUPS
    earlier = (iota((tok, tok), 0) < iota((tok, tok), 1)).astype(BF16)
    e_io = iota((experts, tok), 0)
    named = jnp.zeros((experts, tok), F32)
    for k in range(top):
        named = named + (e_io == r_k[k]).astype(F32)
    rank = mm(named.astype(BF16), earlier)
    g_io = iota((16, tok), 0)
    in_group = (g_io == g_t).astype(F32)
    g_rank = mm(in_group.astype(BF16), earlier)
    pos = jnp.sum(in_group * g_rank, axis=0, keepdims=True).astype(I32)
    for k in range(top):
        rank_k = jnp.sum(jnp.where(e_io == r_k[k], rank, 0.0), axis=0, keepdims=True)
        sq_out[k : k + 1, :] = ((r_k[k] - g_t * epg) * cap + 1).astype(F32) + rank_k
        sq_out[top + k : top + k + 1, :] = prob[k : k + 1, :]
    wide = 2 * gmax
    wr = iota((GROUPS * wide, tok), 0)
    sel2 = (wr == g_t * wide + pos) | (wr == g_t * wide + gmax + pos)
    meta = lax.dot_general(
        sq_out[0 : 2 * top, :], sel2.astype(F32), (((1,), (1,)), ((), ())),
        preferred_element_type=F32, precision=lax.Precision.HIGHEST,
    )
    for g in range(GROUPS):
        meta_out[g] = meta[:, g * wide : (g + 1) * wide]
    place[...] = (iota((GROUPS * gmax, tok), 0) == g_t * gmax + pos).astype(BF16)

    floats = tokens[...].astype(F32)
    inv = lax.rsqrt(jnp.mean(floats * floats, axis=-1, keepdims=True) + EPS)
    normed = (tokens[:, my_cols].astype(F32) * inv * gain[:, my_cols]).astype(BF16)
    packed[...] = mm(place[...], normed).astype(BF16).reshape(packed.shape)

    pl.semaphore_wait(barrier, (lines - 1) + (cols - 1) + 1)

    def rel(a):
        return lax.rem(a + 2 * GROUPS, GROUPS)

    def meta_copy(j):
        zt = lax.rem(z + j, lines)
        gt = lax.div(zt, deep)
        return remote(
            meta_out.at[gt], meta_in.at[rel(grp - gt), o], m_send.at[j], m_recv.at[j], at_z(zt)
        )

    for j in range(1, lines):
        meta_copy(j).start()

    def chunk(d, s):
        return zbuf.at[d, lax.div(s, two), lax.rem(s, two)]

    def first(t, row):
        gt = lax.rem(grp + t, GROUPS)
        d = (GROUPS - t) % GROUPS
        return remote(
            packed.at[gt], chunk(d, o), i_send.at[t], z_recv.at[d, o], at_z(gt * deep + row)
        )

    opp = first(2, (deep - 1) * (1 - late))
    nxt = first(1, 0)
    prv = first(3, deep - 1)
    own_up = remote(packed.at[grp], chunk(0, o), i_send.at[0], z_recv.at[0, o], at_z(lax.rem(z + 1, lines)))
    own_dn = remote(packed.at[grp], chunk(0, o), i_send.at[4], z_recv.at[0, o], at_z(lax.rem(z + lines - 1, lines)))
    pl.when(o < deep - 1)(own_up.start)
    pl.when(o > 0)(own_dn.start)
    nxt.start()
    prv.start()
    wd_copy = remote(wd_hbm.at[:, :, peer_cols], wd.at[core], wd_send.at[0], wd_recv.at[0], other_core)
    wd_copy.start()
    zbuf[0, late, lax.rem(o, two)] = packed[grp]
    meta_in[0, o] = meta_out[grp]

    def onward(plus):
        zz = lax.rem(z + plus * 2 - 1 + lines, lines)
        more = ((plus == 1) & (o < deep - 1)) | ((plus == 0) & (o > 0))
        return zz, more

    def z_copy(d, s, plus):
        zz, more = onward(plus)
        return remote(chunk(d, s), chunk(d, s), z_send.at[d, s], z_recv.at[d, s], at_z(zz)), more

    def arrive(d, s, plus):
        copy, more = z_copy(d, s, plus)
        copy.wait_recv()
        pl.when(more)(copy.start)

    pair = two * gmax
    run = two * cap

    def x_to(src, dst, send, recv, d, h, j):
        xx = lax.rem(x + j, cols)
        return remote(src.at[d, h, xx], dst.at[d, h, x], send.at[d, h, j], recv.at[d, h, j], at_x(xx))

    def x_from(src, dst, send, recv, d, h, j):
        xx = lax.rem(x + cols - j, cols)
        return remote(src.at[d, h, xx], dst.at[d, h, xx], send.at[d, h, j], recv.at[d, h, j], at_x(xx))

    out_args = (xsend, rows.at[core], x_send, x_recv)
    back_args = (back_out, back_in, b_send, b_recv)
    x_order = [1, cols - 1] + list(range(2, cols - 1))

    def d_copy(d, h):
        return remote(rows.at[core, d, h], rows.at[core, d, h], d_send.at[d, h], d_recv.at[d, h], other_core)

    def d_arrival(d, h):
        return remote(rows.at[peer, d, h], rows.at[peer, d, h], d_send.at[d, h], d_recv.at[d, h], other_core)

    def select(d, h):
        lane = iota((2 * top, 2 * gmax), 1)
        info = jnp.where(lane < gmax, meta_in[d, two * h], meta_in[d, two * h + 1])
        zs = lax.div(iota((1, pair), 1), gmax)
        s_io = iota((pair, pair), 0)
        a = jnp.zeros((pair, pair), F32)
        w = jnp.zeros((pair, pair), F32)
        span = cols * loc * cap
        for k in range(top):
            v = info[k : k + 1, :].astype(I32) - 1 - span * o
            ok = (v >= 0) & (v < span)
            sid = jnp.where(ok, lax.div(v, cap) * run + zs * cap + lax.rem(v, cap), -1)
            hit = s_io == sid
            a = jnp.where(hit, 1.0, a)
            w = jnp.where(hit, info[top + k : top + k + 1, :], w)
        picked = mm(a.astype(BF16), zbuf[d, h].reshape(pair, half)).astype(BF16)
        xsend[d, h] = picked.reshape(cols, loc * run, half)
        for j in x_order:
            x_to(*out_args, d, h, j).start()
        rows[core, d, h, x] = xsend[d, h, x]
        hi = w.astype(BF16)
        mix_hi[d, h] = hi
        mix_lo[d, h] = (w - hi.astype(F32)).astype(BF16)

    def exchange(d, h):
        for j in x_order:
            x_from(*out_args, d, h, j).wait_recv()
        d_copy(d, h).start()

    m = cols * run

    def h_copy(d, h):
        return remote(hid.at[core, d, h], hid.at[core, d, h], h_send.at[d, h], h_recv.at[d, h], other_core)

    def h_arrival(d, h):
        return remote(hid.at[peer, d, h], hid.at[peer, d, h], h_send.at[d, h], h_recv.at[d, h], other_core)

    def gate_up(d, h):
        d_arrival(d, h).wait_recv()
        for e in range(loc):
            r = [rows[c, d, h, :, e * run : (e + 1) * run, :].reshape(m, half) for c in range(2)]
            ga = mm(r[0], wg[e, :half, :]) + mm(r[1], wg[e, half:, :])
            up = mm(r[0], wu[e, :half, :]) + mm(r[1], wu[e, half:, :])
            hid[core, d, h, e] = (ga / (1.0 + jnp.exp(-ga)) * up).astype(BF16)
        h_copy(d, h).start()

    def down(d, h):
        h_arrival(d, h).wait_recv()
        for e in range(loc):
            y = mm(hid[0, d, h, e], wd[0, e]) + mm(hid[1, d, h, e], wd[1, e])
            back_out[d, h, :, e * run : (e + 1) * run, :] = y.astype(BF16).reshape(cols, run, half)
        for j in x_order:
            x_to(*back_args, d, h, j).start()
        back_in[d, h, x] = back_out[d, h, x]

    def combine(d, h):
        for j in x_order:
            x_from(*back_args, d, h, j).wait_recv()
        res = back_in[d, h].reshape(pair, half)
        part[d, h] = mm_tn(mix_hi[d, h], res) + mm_tn(mix_lo[d, h], res)

    def home_copy(d, s, plus):
        direct = (deep - 1) * (1 - plus)
        gs = lax.rem(grp + d, GROUPS)
        return remote(
            psend.at[d, s], ret.at[grp], p_send.at[d, s], ret_recv.at[lax.rem(GROUPS - d, GROUPS)],
            at_z(gs * deep + s),
        ), o == direct

    def chain_copy(d, s, plus):
        zz = lax.rem(z - (plus * 2 - 1) + lines, lines)
        return remote(psend.at[d, s], rz.at[d, s], p_send.at[d, s], c_recv.at[d, s], at_z(zz))

    def side_copy(s, plus):
        zz = lax.rem(z - (plus * 2 - 1) + lines, lines)
        return remote(psend.at[0, s], side.at[1 - plus], p_send.at[0, s], side_recv.at[1 - plus], at_z(zz))

    def mine(d, s):
        at = pl.multiple_of(lax.rem(s, two) * gmax, gmax)
        return part[d, lax.div(s, two), pl.ds(at, gmax), :]

    def send_back(d, s, plus):
        _, more = onward(plus)

        @pl.when(more)
        def _():
            chain_copy(d, s, plus).wait_recv()
            psend[d, s] = (mine(d, s) + rz[d, s].astype(F32)).astype(BF16)

        @pl.when(jnp.logical_not(more))
        def _():
            psend[d, s] = mine(d, s).astype(BF16)

        own = d == 0
        home, last = home_copy(d, s, plus)
        near = s + plus * 2 - 1 == o
        to_home = jnp.logical_not(own) & last
        to_side = own & near
        pl.when(to_home)(home.start)
        pl.when(to_side)(side_copy(s, plus).start)
        pl.when(jnp.logical_not(to_home | to_side))(chain_copy(d, s, plus).start)

    def mirrored(kind, d, s):
        return kind, (GROUPS - d) % GROUPS, (deep if kind in (ARRIVE, BACK) else 2) - 1 - s

    def pick(values):
        if len(set(values)) == 1:
            return jnp.int32(values[0])
        return sum(i * v for i, v in zip(in_row, values))

    def way(d, s, r):
        return {3: 1, 1: 0, 2: int(s >= two), 0: int(s < r)}[d]

    for n, (kind, d0, s0, d1, s1) in enumerate(PLAN):
        if kind == WAIT_META:
            for j in range(1, lines):
                meta_copy(j).wait_recv()
            continue
        if kind == WAIT_W:
            for copy in w_copies:
                copy.wait()
            remote(
                wd_hbm.at[:, :, my_cols], wd.at[peer], wd_send.at[0], wd_recv.at[0], other_core
            ).wait_recv()
            continue
        if kind == SEND_OPP:
            opp.start()
            continue
        per_row = [(d0, s0), (d1, s1)]
        per_row += [mirrored(kind, *p)[1:] for p in per_row[::-1]]
        d, s = pick([p[0] for p in per_row]), pick([p[1] for p in per_row])
        if kind in (ARRIVE, BACK):
            plus = pick([way(*p, r) for r, p in enumerate(per_row)])
            (arrive if kind == ARRIVE else send_back)(d, s, plus)
        else:
            {SELECT: select, EXCHANGE: exchange, GATE_UP: gate_up, DOWN: down, COMBINE: combine}[kind](d, s)

    for t in range(1, GROUPS):
        gt = lax.rem(grp + t, GROUPS)
        remote(psend.at[t, o], ret.at[gt], p_send.at[t, o], ret_recv.at[t], at_z(z)).wait_recv()

    @pl.when(o < deep - 1)
    def _():
        side_copy(o, 1).wait_recv()

    @pl.when(o > 0)
    def _():
        side_copy(o, 0).wait_recv()

    own = mine(0, o)
    own = own + jnp.where(o < deep - 1, side[0].astype(F32), 0.0)
    own = own + jnp.where(o > 0, side[1].astype(F32), 0.0)
    ret[grp] = own.astype(BF16)
    mixed = mm_tn(place[...], ret[...].reshape(GROUPS * gmax, half))
    sq = jnp.zeros((tok, 128), F32)
    for i in range(half // 128):
        v = mixed[:, i * 128 : (i + 1) * 128]
        sq = sq + v * v
    sq_out[...] = sq
    q_copy = remote(sq_out, sq_in, q_send.at[0], q_recv.at[0], other_core)
    q_copy.start()
    q_copy.wait_recv()
    total = jnp.sum(sq_out[...] + sq_in[...], axis=1, keepdims=True)
    out_ref[...] = (mixed * lax.rsqrt(total / width + EPS) * out_gain[...]).astype(BF16)

    q_copy.wait_send()
    for j in range(1, lines):
        meta_copy(j).wait_send()
    opp.wait_send()
    nxt.wait_send()
    prv.wait_send()
    pl.when(o < deep - 1)(own_up.wait_send)
    pl.when(o > 0)(own_dn.wait_send)
    wd_copy.wait_send()

    def sent(d, s, plus):
        copy, more = z_copy(d, s, plus)
        pl.when(more)(copy.wait_send)
        chain_copy(d, s, plus).wait_send()

    for s in range(deep):
        sent(2, s, s // two)
        sent(3, s, 1)
        sent(1, s, 0)
    for j in range(1, deep):
        s = lax.rem(o + j, deep)
        sent(0, s, (s < o).astype(I32))
    for d in range(GROUPS):
        for h in range(2):
            h_copy(d, h).wait_send()
            d_copy(d, h).wait_send()
            for j in range(1, cols):
                x_to(*out_args, d, h, j).wait_send()
                x_to(*back_args, d, h, j).wait_send()


def body(tokens, in_gain, routing, gate_prob, w_gate, w_up, w_down, out_gain):
    ep_count = lax.axis_size("ep")
    loc, width, ff = w_gate.shape
    tok, top = routing.shape
    half = out_gain.shape[0]
    epg = loc * ep_count // GROUPS
    cap = max(2, tok * top // (2 * epg))
    gmax = epg * cap // top
    side = math.isqrt(ep_count // GROUPS)
    lines = ep_count // side
    cols, deep = side, side
    two = deep // 2
    pair = two * gmax
    piece = loc * two * cap
    m = cols * two * cap
    cfg = (lines, side, tok, top, cap, gmax, half, width, epg)
    vmem = pl.BlockSpec(memory_space=pltpu.VMEM)
    anyw = pl.BlockSpec(memory_space=pl.ANY)
    dma = pltpu.SemaphoreType.DMA
    scratch = [
        pltpu.VMEM(w_gate.shape, BF16),
        pltpu.VMEM(w_up.shape, BF16),
        pltpu.VMEM((2, loc, ff, half), BF16),
        pltpu.VMEM((GROUPS * gmax, tok), BF16),
        pltpu.VMEM((GROUPS, 2 * top, 2 * gmax), F32),
        pltpu.VMEM((GROUPS, deep, 2 * top, 2 * gmax), F32),
        pltpu.VMEM((GROUPS, gmax, half), BF16),
        pltpu.VMEM((GROUPS, 2, two, gmax, half), BF16),
        pltpu.VMEM((GROUPS, 2, pair, pair), BF16),
        pltpu.VMEM((GROUPS, 2, pair, pair), BF16),
        pltpu.VMEM((GROUPS, 2, cols, piece, half), BF16),
        pltpu.VMEM((2, GROUPS, 2, cols, piece, half), BF16),
        pltpu.VMEM((2, GROUPS, 2, loc, m, ff), BF16),
        pltpu.VMEM((GROUPS, 2, cols, piece, half), BF16),
        pltpu.VMEM((GROUPS, 2, cols, piece, half), BF16),
        pltpu.VMEM((GROUPS, 2, pair, half), F32),
        pltpu.VMEM((GROUPS, deep, gmax, half), BF16),
        pltpu.VMEM((GROUPS, deep, gmax, half), BF16),
        pltpu.VMEM((2, gmax, half), BF16),
        pltpu.VMEM((GROUPS, gmax, half), BF16),
        pltpu.VMEM((tok, 128), F32),
        pltpu.VMEM((tok, 128), F32),
        dma((3,)),
        dma((1,)),
        dma((1,)),
        dma((lines,)),
        dma((lines,)),
        dma((5,)),
        dma((GROUPS, deep)),
        dma((GROUPS, deep)),
        dma((GROUPS, 2, cols)),
        dma((GROUPS, 2, cols)),
        dma((GROUPS, 2)),
        dma((GROUPS, 2)),
        dma((GROUPS, 2)),
        dma((GROUPS, 2)),
        dma((GROUPS, 2, cols)),
        dma((GROUPS, 2, cols)),
        dma((GROUPS, deep)),
        dma((GROUPS, deep)),
        dma((2,)),
        dma((GROUPS,)),
        dma((1,)),
        dma((1,)),
    ]
    return pl.pallas_call(
        functools.partial(kernel, cfg),
        out_shape=jax.ShapeDtypeStruct((tok, half), BF16),
        in_specs=[vmem] * 5 + [anyw] * 3,
        out_specs=vmem,
        scratch_shapes=scratch,
        compiler_params=pltpu.CompilerParams(
            collective_id=0, has_side_effects=True, vmem_limit_bytes=60 * 1024 * 1024
        ),
    )(
        routing.T, gate_prob.T, tokens, in_gain.reshape(1, width), out_gain.reshape(1, half),
        w_gate, w_up, w_down,
    )


def solution(mesh):
    placed = (
        P(("grp", "ep"), None),
        P(),
        P(("grp", "ep"), None),
        P(("grp", "ep"), None),
        P("ep", None, "tp"),
        P("ep", None, "tp"),
        P("ep", "tp", None),
        P("tp"),
    )
    return jax.shard_map(
        body, mesh=mesh, in_specs=placed, out_specs=P(("grp", "ep"), "tp"), check_vma=False
    )
```

```python
import functools
import math

import jax
import jax.numpy as jnp
from jax import lax
from jax.experimental import pallas as pl
from jax.experimental.pallas import tpu as pltpu
from jax.sharding import PartitionSpec as P

GROUPS = 4
EPS = 1e-06
MESH = pl.DeviceIdType.MESH
F32 = jnp.float32
BF16 = jnp.bfloat16
I32 = jnp.int32


def iota(shape, dim):
    return lax.broadcasted_iota(I32, shape, dim)


def mm(a, b):
    return jnp.dot(a, b, preferred_element_type=F32)


def mm_tn(a, b):
    return lax.dot_general(a, b, (((0,), (0,)), ((), ())), preferred_element_type=F32)


PARTS = 2
ARRIVE, BACK, SELECT, EXCHANGE, GATE_UP, DOWN, COMBINE, SEND, WAIT_META, WAIT_W = range(10)

PLAN = (
    (SEND, 0, 0, 0, 0), (SEND, 1, 0, 1, 0), (SEND, 3, 0, 3, 0), (ARRIVE, 0, 1, 0, 2),
    (ARRIVE, 3, 3, 0, 0), (WAIT_META, 0, 0, 0, 0), (SELECT, 0, 0, 0, 0), (EXCHANGE, 0, 0, 0, 0),
    (WAIT_W, 0, 0, 0, 0), (GATE_UP, 0, 0, 0, 0), (DOWN, 0, 0, 0, 0), (ARRIVE, 3, 2, 3, 3),
    (ARRIVE, 3, 1, 0, 3), (SELECT, 3, 1, 0, 1), (SEND, 2, 0, 2, 0), (ARRIVE, 3, 0, 3, 2),
    (SELECT, 3, 0, 3, 1), (COMBINE, 0, 0, 0, 0), (EXCHANGE, 3, 1, 0, 1), (GATE_UP, 3, 1, 0, 1),
    (DOWN, 3, 1, 0, 1), (ARRIVE, 0, 2, 3, 1), (ARRIVE, 0, 3, 1, 0), (EXCHANGE, 3, 0, 3, 1),
    (GATE_UP, 3, 0, 3, 1), (DOWN, 3, 0, 3, 1), (ARRIVE, 2, 3, 1, 1), (SELECT, 0, 1, 1, 0),
    (COMBINE, 3, 1, 0, 1), (ARRIVE, 1, 0, 3, 0), (ARRIVE, 2, 2, 1, 2), (SELECT, 2, 1, 3, 0),
    (COMBINE, 3, 0, 3, 1), (ARRIVE, 1, 1, 1, 3), (ARRIVE, 1, 2, 2, 3), (EXCHANGE, 0, 1, 1, 0),
    (SELECT, 1, 0, 1, 1), (ARRIVE, 1, 3, 2, 2), (SELECT, 1, 1, 2, 1), (GATE_UP, 0, 1, 1, 0),
    (ARRIVE, 2, 0, 2, 0), (EXCHANGE, 2, 1, 3, 0), (DOWN, 0, 1, 1, 0), (ARRIVE, 2, 1, 2, 1),
    (SELECT, 2, 0, 2, 0), (EXCHANGE, 1, 0, 1, 1), (GATE_UP, 1, 0, 3, 0), (EXCHANGE, 1, 1, 2, 1),
    (GATE_UP, 2, 1, 1, 1), (DOWN, 2, 1, 3, 0), (BACK, 0, 1, 0, 2), (DOWN, 1, 0, 1, 1),
    (GATE_UP, 1, 1, 2, 1), (COMBINE, 0, 1, 1, 0), (BACK, 0, 2, 0, 3), (BACK, 0, 3, 0, 0),
    (DOWN, 1, 1, 2, 1), (EXCHANGE, 2, 0, 2, 0), (COMBINE, 1, 0, 1, 1), (BACK, 1, 1, 1, 1),
    (GATE_UP, 2, 0, 2, 0), (BACK, 1, 0, 1, 0), (DOWN, 2, 0, 2, 0), (COMBINE, 2, 1, 2, 1),
    (COMBINE, 1, 1, 3, 0), (BACK, 1, 3, 3, 2), (BACK, 1, 2, 1, 3), (COMBINE, 2, 0, 2, 0),
    (BACK, 2, 0, 3, 3), (BACK, 2, 1, 1, 2), (BACK, 3, 2, 3, 0), (BACK, 3, 3, 2, 0),
    (BACK, 3, 0, 3, 1), (BACK, 3, 1, 2, 1), (BACK, 2, 2, 2, 2), (BACK, 2, 3, 2, 3),
)


def kernel(
    cfg, routing, prob, tokens, gain, out_gain, wg_hbm, wu_hbm, wd_hbm, out_ref,
    wg, wu, wd, place, meta_out, meta_in, packed, zbuf, mix_hi, mix_lo, xsend, rows, hid,
    back_out, back_in, part, psend, land, ret, sq_out, sq_in,
    w_sem, wd_send, wd_recv, m_send, m_recv, i_send, z_send, z_recv, x_send, x_recv,
    d_send, d_recv, h_send, h_recv, b_send, b_recv, p_send, l_recv,
    q_send, q_recv,
):
    lines, side_len, tok, top, cap, gmax, half, width, epg = cfg
    cols, deep = side_len, side_len
    two = deep // 2
    bit = gmax // PARTS
    bits = [pl.ds(q * bit, bit) for q in range(PARTS)]
    home_at, side_at = GROUPS * deep, GROUPS * deep + GROUPS
    me = lax.axis_index("ep")
    core = lax.axis_index("tp")
    peer = 1 - core
    x, z = lax.rem(me, cols), lax.div(me, cols)
    grp, o = lax.div(z, deep), lax.rem(z, deep)
    late = lax.div(o, two)
    in_row = [(o == r).astype(I32) for r in range(deep)]
    loc = wg.shape[0]

    def at_z(zz):
        return {"ep": zz * cols + x}

    def at_x(xx):
        return {"ep": z * cols + xx}

    def remote(src, dst, s, r, dev):
        return pltpu.make_async_remote_copy(
            src_ref=src, dst_ref=dst, send_sem=s, recv_sem=r, device_id=dev, device_id_type=MESH
        )

    other_core = {"tp": peer}
    my_cols = pl.ds(pl.multiple_of(core * half, half), half)
    peer_cols = pl.ds(pl.multiple_of(peer * half, half), half)

    barrier = pltpu.get_barrier_semaphore()
    for j in range(1, lines):
        pl.semaphore_signal(barrier, 1, device_id=at_z(lax.rem(z + j, lines)), device_id_type=MESH)
    for j in range(1, cols):
        pl.semaphore_signal(barrier, 1, device_id=at_x(lax.rem(x + j, cols)), device_id_type=MESH)
    pl.semaphore_signal(barrier, 1, device_id=other_core, device_id_type=MESH)

    w_copies = [
        pltpu.make_async_copy(wg_hbm, wg, w_sem.at[0]),
        pltpu.make_async_copy(wu_hbm, wu, w_sem.at[1]),
        pltpu.make_async_copy(wd_hbm.at[:, :, my_cols], wd.at[core], w_sem.at[2]),
    ]
    for copy in w_copies:
        copy.start()

    r_k = [routing[k : k + 1, :] for k in range(top)]
    g_t = lax.div(r_k[0], epg)
    experts = epg * GROUPS
    earlier = (iota((tok, tok), 0) < iota((tok, tok), 1)).astype(BF16)
    e_io = iota((experts, tok), 0)
    named = jnp.zeros((experts, tok), F32)
    for k in range(top):
        named = named + (e_io == r_k[k]).astype(F32)
    rank = mm(named.astype(BF16), earlier)
    g_io = iota((16, tok), 0)
    in_group = (g_io == g_t).astype(F32)
    g_rank = mm(in_group.astype(BF16), earlier)
    pos = jnp.sum(in_group * g_rank, axis=0, keepdims=True).astype(I32)
    for k in range(top):
        rank_k = jnp.sum(jnp.where(e_io == r_k[k], rank, 0.0), axis=0, keepdims=True)
        sq_out[k : k + 1, :] = ((r_k[k] - g_t * epg) * cap + 1).astype(F32) + rank_k
        sq_out[top + k : top + k + 1, :] = prob[k : k + 1, :]
    wide = 2 * gmax
    wr = iota((GROUPS * wide, tok), 0)
    sel2 = (wr == g_t * wide + pos) | (wr == g_t * wide + gmax + pos)
    meta = lax.dot_general(
        sq_out[0 : 2 * top, :], sel2.astype(F32), (((1,), (1,)), ((), ())),
        preferred_element_type=F32, precision=lax.Precision.HIGHEST,
    )
    for g in range(GROUPS):
        meta_out[g] = meta[:, g * wide : (g + 1) * wide]
    place[...] = (iota((GROUPS * gmax, tok), 0) == g_t * gmax + pos).astype(BF16)

    floats = tokens[...].astype(F32)
    inv = lax.rsqrt(jnp.mean(floats * floats, axis=-1, keepdims=True) + EPS)
    normed = (tokens[:, my_cols].astype(F32) * inv * gain[:, my_cols]).astype(BF16)
    packed[...] = mm(place[...], normed).astype(BF16).reshape(packed.shape)

    pl.semaphore_wait(barrier, (lines - 1) + (cols - 1) + 1)

    def rel(a):
        return lax.rem(a + 2 * GROUPS, GROUPS)

    def meta_copy(j):
        zt = lax.rem(z + j, lines)
        gt = lax.div(zt, deep)
        return remote(
            meta_out.at[gt], meta_in.at[rel(grp - gt), o], m_send.at[j], m_recv.at[j], at_z(zt)
        )

    for j in range(1, lines):
        meta_copy(j).start()

    def chunk(d, s, q):
        return zbuf.at[d, lax.div(s, two), lax.rem(s, two), bits[q]]

    def first(t, row, i, d):
        gt = lax.rem(grp + t, GROUPS)
        return [
            remote(
                packed.at[gt, bits[q]], chunk(d, o, q), i_send.at[i, q], z_recv.at[d, o, q], at_z(row(gt))
            )
            for q in range(PARTS)
        ]

    opp = first(2, lambda gt: gt * deep + (deep - 1) * (1 - late), 2, 2)
    nxt = first(1, lambda gt: gt * deep, 1, 3)
    prv = first(3, lambda gt: gt * deep + deep - 1, 3, 1)
    own_up = first(0, lambda gt: lax.rem(z + 1, lines), 0, 0)
    own_dn = first(0, lambda gt: lax.rem(z + lines - 1, lines), 4, 0)

    def each(copies, what):
        def run_all():
            for copy in copies:
                getattr(copy, what)()

        return run_all

    wd_copy = remote(wd_hbm.at[:, :, peer_cols], wd.at[core], wd_send.at[0], wd_recv.at[0], other_core)
    wd_copy.start()
    zbuf[0, late, lax.rem(o, two)] = packed[grp]
    meta_in[0, o] = meta_out[grp]

    def onward(plus):
        zz = lax.rem(z + plus * 2 - 1 + lines, lines)
        more = ((plus == 1) & (o < deep - 1)) | ((plus == 0) & (o > 0))
        return zz, more

    def z_copy(d, s, plus, q):
        zz, more = onward(plus)
        here = chunk(d, s, q)
        return remote(here, here, z_send.at[d, s, q], z_recv.at[d, s, q], at_z(zz)), more

    def arrive(d, s, plus):
        for q in range(PARTS):
            copy, more = z_copy(d, s, plus, q)
            copy.wait_recv()
            pl.when(more)(copy.start)

    pair = two * gmax
    run = two * cap

    def x_to(src, dst, send, recv, d, h, j):
        xx = lax.rem(x + j, cols)
        return remote(src.at[d, h, xx], dst.at[d, h, x], send.at[d, h, j], recv.at[d, h, j], at_x(xx))

    def x_from(src, dst, send, recv, d, h, j):
        xx = lax.rem(x + cols - j, cols)
        return remote(src.at[d, h, xx], dst.at[d, h, xx], send.at[d, h, j], recv.at[d, h, j], at_x(xx))

    out_args = (xsend, rows.at[core], x_send, x_recv)
    back_args = (back_out, back_in, b_send, b_recv)
    x_order = [1, cols - 1] + list(range(2, cols - 1))

    def d_copy(d, h):
        return remote(rows.at[core, d, h], rows.at[core, d, h], d_send.at[d, h], d_recv.at[d, h], other_core)

    def d_arrival(d, h):
        return remote(rows.at[peer, d, h], rows.at[peer, d, h], d_send.at[d, h], d_recv.at[d, h], other_core)

    def select(d, h):
        lane = iota((2 * top, 2 * gmax), 1)
        info = jnp.where(lane < gmax, meta_in[d, two * h], meta_in[d, two * h + 1])
        zs = lax.div(iota((1, pair), 1), gmax)
        s_io = iota((pair, pair), 0)
        a = jnp.zeros((pair, pair), F32)
        w = jnp.zeros((pair, pair), F32)
        span = cols * loc * cap
        for k in range(top):
            v = info[k : k + 1, :].astype(I32) - 1 - span * o
            ok = (v >= 0) & (v < span)
            sid = jnp.where(ok, lax.div(v, cap) * run + zs * cap + lax.rem(v, cap), -1)
            hit = s_io == sid
            a = jnp.where(hit, 1.0, a)
            w = jnp.where(hit, info[top + k : top + k + 1, :], w)
        picked = mm(a.astype(BF16), zbuf[d, h].reshape(pair, half)).astype(BF16)
        xsend[d, h] = picked.reshape(cols, loc * run, half)
        for j in x_order:
            x_to(*out_args, d, h, j).start()
        rows[core, d, h, x] = xsend[d, h, x]
        hi = w.astype(BF16)
        mix_hi[d, h] = hi
        mix_lo[d, h] = (w - hi.astype(F32)).astype(BF16)

    def exchange(d, h):
        for j in x_order:
            x_from(*out_args, d, h, j).wait_recv()
        d_copy(d, h).start()

    m = cols * run

    def h_copy(d, h):
        return remote(hid.at[core, d, h], hid.at[core, d, h], h_send.at[d, h], h_recv.at[d, h], other_core)

    def h_arrival(d, h):
        return remote(hid.at[peer, d, h], hid.at[peer, d, h], h_send.at[d, h], h_recv.at[d, h], other_core)

    def gate_up(d, h):
        d_arrival(d, h).wait_recv()
        for e in range(loc):
            r = [rows[c, d, h, :, e * run : (e + 1) * run, :].reshape(m, half) for c in range(2)]
            ga = mm(r[0], wg[e, :half, :]) + mm(r[1], wg[e, half:, :])
            up = mm(r[0], wu[e, :half, :]) + mm(r[1], wu[e, half:, :])
            hid[core, d, h, e] = (ga / (1.0 + jnp.exp(-ga)) * up).astype(BF16)
        h_copy(d, h).start()

    def down(d, h):
        h_arrival(d, h).wait_recv()
        for e in range(loc):
            y = mm(hid[0, d, h, e], wd[0, e]) + mm(hid[1, d, h, e], wd[1, e])
            back_out[d, h, :, e * run : (e + 1) * run, :] = y.astype(BF16).reshape(cols, run, half)
        for j in x_order:
            x_to(*back_args, d, h, j).start()
        back_in[d, h, x] = back_out[d, h, x]

    def combine(d, h):
        for j in x_order:
            x_from(*back_args, d, h, j).wait_recv()
        res = back_in[d, h].reshape(pair, half)
        part[d, h] = mm_tn(mix_hi[d, h], res) + mm_tn(mix_lo[d, h], res)

    def landing(d, s, q, at, zz):
        return remote(
            psend.at[d, s, bits[q]], land.at[at, bits[q]], p_send.at[d, s, q], l_recv.at[at, q], at_z(zz)
        )

    def mine(d, s, q):
        at = pl.multiple_of(lax.rem(s, two) * gmax + q * bit, bit)
        return part[d, lax.div(s, two), pl.ds(at, bit), :]

    def send_back(d, s, plus):
        _, more = onward(plus)
        own = (d == 0).astype(I32)
        home = (1 - own) * (o == (deep - 1) * (1 - plus)).astype(I32)
        near = own * (s + plus * 2 - 1 == o).astype(I32)
        chain = d * deep + s
        at = home * (home_at + grp) + near * (side_at + 1 - plus) + (1 - home - near) * chain
        beside = lax.rem(z - (plus * 2 - 1) + lines, lines)
        zz = home * (lax.rem(grp + d, GROUPS) * deep + s) + (1 - home) * beside
        for q in range(PARTS):

            @pl.when(more)
            def _():
                landing(d, s, q, chain, z).wait_recv()
                psend[d, s, bits[q]] = (mine(d, s, q) + land[chain, bits[q]].astype(F32)).astype(BF16)

            @pl.when(jnp.logical_not(more))
            def _():
                psend[d, s, bits[q]] = mine(d, s, q).astype(BF16)

            landing(d, s, q, at, zz).start()

    def mirrored(kind, d, s):
        return (GROUPS - d) % GROUPS, (deep if kind in (ARRIVE, BACK) else 2) - 1 - s

    def pick(values):
        if len(set(values)) == 1:
            return jnp.int32(values[0])
        return sum(i * v for i, v in zip(in_row, values))

    def way(d, s, r):
        return {3: 1, 1: 0, 2: int(s >= two), 0: int(s < r)}[d]

    for n, (kind, d0, s0, d1, s1) in enumerate(PLAN):
        if kind == WAIT_META:
            for j in range(1, lines):
                meta_copy(j).wait_recv()
            continue
        if kind == WAIT_W:
            for copy in w_copies:
                copy.wait()
            remote(
                wd_hbm.at[:, :, my_cols], wd.at[peer], wd_send.at[0], wd_recv.at[0], other_core
            ).wait_recv()
            continue
        per_row = [(d0, s0), (d1, s1)]
        per_row += [mirrored(kind, *p) for p in per_row[::-1]]
        if kind == SEND:
            for t, copies in ((1, nxt), (2, opp), (3, prv)):
                flags = [int(p[0] == t) for p in per_row]
                if all(flags):
                    each(copies, "start")()
                elif any(flags):
                    pl.when(pick(flags) == 1)(each(copies, "start"))
            flags = [int(p[0] == 0) for p in per_row]
            if any(flags):
                pl.when((pick(flags) == 1) & (o < deep - 1))(each(own_up, "start"))
                pl.when((pick(flags) == 1) & (o > 0))(each(own_dn, "start"))
            continue
        d, s = pick([p[0] for p in per_row]), pick([p[1] for p in per_row])
        if kind in (ARRIVE, BACK):
            plus = pick([way(*p, r) for r, p in enumerate(per_row)])
            (arrive if kind == ARRIVE else send_back)(d, s, plus)
        else:
            {SELECT: select, EXCHANGE: exchange, GATE_UP: gate_up, DOWN: down, COMBINE: combine}[kind](d, s)

    own = jnp.concatenate([mine(0, o, q) for q in range(PARTS)], axis=0)

    @pl.when(o < deep - 1)
    def _():
        for q in range(PARTS):
            landing(0, o, q, side_at, z).wait_recv()

    @pl.when(o > 0)
    def _():
        for q in range(PARTS):
            landing(0, o, q, side_at + 1, z).wait_recv()

    own = own + jnp.where(o < deep - 1, land[side_at].astype(F32), 0.0)
    own = own + jnp.where(o > 0, land[side_at + 1].astype(F32), 0.0)
    for t in (1, 3, 2):
        gt = lax.rem(grp + t, GROUPS)
        for q in range(PARTS):
            landing(0, o, q, home_at + gt, z).wait_recv()
    ret[...] = land[home_at : home_at + GROUPS]
    ret[grp] = own.astype(BF16)
    mixed = mm_tn(place[...], ret[...].reshape(GROUPS * gmax, half))
    sq = jnp.zeros((tok, 128), F32)
    for i in range(half // 128):
        v = mixed[:, i * 128 : (i + 1) * 128]
        sq = sq + v * v
    sq_out[...] = sq
    q_copy = remote(sq_out, sq_in, q_send.at[0], q_recv.at[0], other_core)
    q_copy.start()
    q_copy.wait_recv()
    total = jnp.sum(sq_out[...] + sq_in[...], axis=1, keepdims=True)
    out_ref[...] = (mixed * lax.rsqrt(total / width + EPS) * out_gain[...]).astype(BF16)

    q_copy.wait_send()
    for j in range(1, lines):
        meta_copy(j).wait_send()
    each(opp + nxt + prv, "wait_send")()
    pl.when(o < deep - 1)(each(own_up, "wait_send"))
    pl.when(o > 0)(each(own_dn, "wait_send"))
    wd_copy.wait_send()

    def sent(d, s, plus):
        copies, more = [z_copy(d, s, plus, q)[0] for q in range(PARTS)], onward(plus)[1]
        pl.when(more)(each(copies, "wait_send"))
        for q in range(PARTS):
            landing(d, s, q, 0, z).wait_send()

    for s in range(deep):
        sent(2, s, s // two)
        sent(3, s, 1)
        sent(1, s, 0)
    for j in range(1, deep):
        s = lax.rem(o + j, deep)
        sent(0, s, (s < o).astype(I32))
    for d in range(GROUPS):
        for h in range(2):
            h_copy(d, h).wait_send()
            d_copy(d, h).wait_send()
            for j in range(1, cols):
                x_to(*out_args, d, h, j).wait_send()
                x_to(*back_args, d, h, j).wait_send()


def body(tokens, in_gain, routing, gate_prob, w_gate, w_up, w_down, out_gain):
    ep_count = lax.axis_size("ep")
    loc, width, ff = w_gate.shape
    tok, top = routing.shape
    half = out_gain.shape[0]
    epg = loc * ep_count // GROUPS
    cap = max(2, tok * top // (2 * epg))
    gmax = epg * cap // top
    side = math.isqrt(ep_count // GROUPS)
    lines = ep_count // side
    cols, deep = side, side
    two = deep // 2
    pair = two * gmax
    piece = loc * two * cap
    m = cols * two * cap
    cfg = (lines, side, tok, top, cap, gmax, half, width, epg)
    vmem = pl.BlockSpec(memory_space=pltpu.VMEM)
    anyw = pl.BlockSpec(memory_space=pl.ANY)
    dma = pltpu.SemaphoreType.DMA
    scratch = [
        pltpu.VMEM(w_gate.shape, BF16),
        pltpu.VMEM(w_up.shape, BF16),
        pltpu.VMEM((2, loc, ff, half), BF16),
        pltpu.VMEM((GROUPS * gmax, tok), BF16),
        pltpu.VMEM((GROUPS, 2 * top, 2 * gmax), F32),
        pltpu.VMEM((GROUPS, deep, 2 * top, 2 * gmax), F32),
        pltpu.VMEM((GROUPS, gmax, half), BF16),
        pltpu.VMEM((GROUPS, 2, two, gmax, half), BF16),
        pltpu.VMEM((GROUPS, 2, pair, pair), BF16),
        pltpu.VMEM((GROUPS, 2, pair, pair), BF16),
        pltpu.VMEM((GROUPS, 2, cols, piece, half), BF16),
        pltpu.VMEM((2, GROUPS, 2, cols, piece, half), BF16),
        pltpu.VMEM((2, GROUPS, 2, loc, m, ff), BF16),
        pltpu.VMEM((GROUPS, 2, cols, piece, half), BF16),
        pltpu.VMEM((GROUPS, 2, cols, piece, half), BF16),
        pltpu.VMEM((GROUPS, 2, pair, half), F32),
        pltpu.VMEM((GROUPS, deep, gmax, half), BF16),
        pltpu.VMEM((GROUPS * deep + GROUPS + 2, gmax, half), BF16),
        pltpu.VMEM((GROUPS, gmax, half), BF16),
        pltpu.VMEM((tok, 128), F32),
        pltpu.VMEM((tok, 128), F32),
        dma((3,)),
        dma((1,)),
        dma((1,)),
        dma((lines,)),
        dma((lines,)),
        dma((5, PARTS)),
        dma((GROUPS, deep, PARTS)),
        dma((GROUPS, deep, PARTS)),
        dma((GROUPS, 2, cols)),
        dma((GROUPS, 2, cols)),
        dma((GROUPS, 2)),
        dma((GROUPS, 2)),
        dma((GROUPS, 2)),
        dma((GROUPS, 2)),
        dma((GROUPS, 2, cols)),
        dma((GROUPS, 2, cols)),
        dma((GROUPS, deep, PARTS)),
        dma((GROUPS * deep + GROUPS + 2, PARTS)),
        dma((1,)),
        dma((1,)),
    ]
    return pl.pallas_call(
        functools.partial(kernel, cfg),
        out_shape=jax.ShapeDtypeStruct((tok, half), BF16),
        in_specs=[vmem] * 5 + [anyw] * 3,
        out_specs=vmem,
        scratch_shapes=scratch,
        compiler_params=pltpu.CompilerParams(
            collective_id=0, has_side_effects=True, vmem_limit_bytes=60 * 1024 * 1024
        ),
    )(
        routing.T, gate_prob.T, tokens, in_gain.reshape(1, width), out_gain.reshape(1, half),
        w_gate, w_up, w_down,
    )


def solution(mesh):
    placed = (
        P(("grp", "ep"), None),
        P(),
        P(("grp", "ep"), None),
        P(("grp", "ep"), None),
        P("ep", None, "tp"),
        P("ep", None, "tp"),
        P("ep", "tp", None),
        P("tp"),
    )
    return jax.shard_map(
        body, mesh=mesh, in_specs=placed, out_specs=P(("grp", "ep"), "tp"), check_vma=False
    )
```

```python
import functools
import math

import jax
import jax.numpy as jnp
from jax import lax
from jax.experimental import pallas as pl
from jax.experimental.pallas import tpu as pltpu
from jax.sharding import PartitionSpec as P

GROUPS = 4
EPS = 1e-06
MESH = pl.DeviceIdType.MESH
F32 = jnp.float32
BF16 = jnp.bfloat16
I32 = jnp.int32


def iota(shape, dim):
    return lax.broadcasted_iota(I32, shape, dim)


def mm(a, b):
    return jnp.dot(a, b, preferred_element_type=F32)


def mm_tn(a, b):
    return lax.dot_general(a, b, (((0,), (0,)), ((), ())), preferred_element_type=F32)


PARTS = 2
ARRIVE, BACK, SELECT, EXCHANGE, GATE_UP, DOWN, COMBINE, SEND, WAIT_META, WAIT_W = range(10)

PLAN = (
    (SEND, 0, 0, 0, 0), (SEND, 3, 0, 3, 0), (ARRIVE, 3, 3, 0, 0), (ARRIVE, 3, 2, 0, 2),
    (ARRIVE, 0, 1, 0, 3), (SEND, 2, 0, 1, 0), (WAIT_META, 0, 0, 0, 0), (SELECT, 0, 0, 0, 0),
    (EXCHANGE, 0, 0, 0, 0), (SEND, 1, 0, 2, 0), (WAIT_W, 0, 0, 0, 0), (GATE_UP, 0, 0, 0, 0),
    (SELECT, 3, 1, 0, 1), (DOWN, 0, 0, 0, 0), (ARRIVE, 3, 0, 3, 3), (EXCHANGE, 3, 1, 0, 1),
    (ARRIVE, 0, 2, 3, 2), (ARRIVE, 3, 1, 1, 0), (ARRIVE, 0, 3, 3, 0), (ARRIVE, 2, 3, 1, 1),
    (SELECT, 3, 0, 3, 1), (SELECT, 0, 1, 1, 0), (ARRIVE, 2, 2, 3, 1), (SELECT, 2, 1, 3, 0),
    (ARRIVE, 1, 0, 1, 3), (ARRIVE, 1, 3, 2, 3), (ARRIVE, 1, 1, 1, 2), (GATE_UP, 3, 1, 0, 1),
    (DOWN, 3, 1, 0, 1), (ARRIVE, 2, 0, 2, 2), (SELECT, 1, 0, 2, 1), (ARRIVE, 1, 2, 2, 0),
    (EXCHANGE, 0, 1, 1, 0), (ARRIVE, 2, 1, 2, 1), (SELECT, 1, 1, 1, 1), (EXCHANGE, 2, 1, 3, 0),
    (GATE_UP, 0, 1, 1, 0), (EXCHANGE, 1, 0, 3, 1), (DOWN, 0, 1, 1, 0), (GATE_UP, 1, 0, 3, 0),
    (EXCHANGE, 1, 1, 1, 1), (COMBINE, 0, 0, 1, 0), (EXCHANGE, 3, 0, 2, 1), (SELECT, 2, 0, 2, 0),
    (GATE_UP, 2, 1, 1, 1), (GATE_UP, 1, 1, 3, 1), (DOWN, 1, 0, 1, 1), (COMBINE, 0, 1, 0, 1),
    (BACK, 0, 3, 0, 3), (EXCHANGE, 2, 0, 2, 0), (DOWN, 1, 1, 3, 1), (BACK, 0, 2, 1, 0),
    (GATE_UP, 3, 0, 2, 0), (COMBINE, 1, 0, 0, 0), (DOWN, 2, 1, 2, 0), (BACK, 1, 0, 1, 1),
    (GATE_UP, 2, 0, 2, 1), (BACK, 1, 1, 0, 2), (DOWN, 2, 0, 2, 1), (COMBINE, 1, 1, 3, 1),
    (BACK, 1, 2, 3, 3), (COMBINE, 2, 0, 2, 0), (DOWN, 3, 0, 3, 0), (BACK, 2, 0, 3, 2),
    (COMBINE, 3, 1, 2, 1), (BACK, 2, 1, 2, 0), (BACK, 1, 3, 0, 0), (COMBINE, 3, 0, 1, 1),
    (BACK, 3, 3, 2, 1), (BACK, 3, 2, 1, 2), (BACK, 0, 1, 2, 3), (COMBINE, 2, 1, 3, 0),
    (BACK, 2, 3, 2, 2), (BACK, 2, 2, 1, 3), (BACK, 3, 1, 3, 1), (BACK, 3, 0, 3, 0),
)


def kernel(
    cfg, routing, prob, tokens, gain, out_gain, wg_hbm, wu_hbm, wd_hbm, out_ref,
    wg, wu, wd, place, meta_out, meta_in, packed, zbuf, mix_hi, mix_lo, xsend, rows, hid,
    back_out, back_in, part, psend, land, ret, sq_out, sq_in,
    w_sem, wd_send, wd_recv, m_send, m_recv, i_send, z_send, z_recv, x_send, x_recv,
    d_send, d_recv, h_send, h_recv, b_send, b_recv, p_send, l_recv,
    q_send, q_recv,
):
    lines, side_len, tok, top, cap, gmax, half, width, epg = cfg
    cols, deep = side_len, side_len
    two = deep // 2
    bit = gmax // PARTS
    bits = [pl.ds(q * bit, bit) for q in range(PARTS)]
    home_at, side_at = GROUPS * deep, GROUPS * deep + GROUPS
    me = lax.axis_index("ep")
    core = lax.axis_index("tp")
    peer = 1 - core
    x, z = lax.rem(me, cols), lax.div(me, cols)
    grp, o = lax.div(z, deep), lax.rem(z, deep)
    late = lax.div(o, two)
    in_row = [(o == r).astype(I32) for r in range(deep)]
    loc = wg.shape[0]

    def at_z(zz):
        return {"ep": zz * cols + x}

    def at_x(xx):
        return {"ep": z * cols + xx}

    def remote(src, dst, s, r, dev):
        return pltpu.make_async_remote_copy(
            src_ref=src, dst_ref=dst, send_sem=s, recv_sem=r, device_id=dev, device_id_type=MESH
        )

    other_core = {"tp": peer}
    my_cols = pl.ds(pl.multiple_of(core * half, half), half)
    peer_cols = pl.ds(pl.multiple_of(peer * half, half), half)

    barrier = pltpu.get_barrier_semaphore()
    for j in range(1, lines):
        pl.semaphore_signal(barrier, 1, device_id=at_z(lax.rem(z + j, lines)), device_id_type=MESH)
    for j in range(1, cols):
        pl.semaphore_signal(barrier, 1, device_id=at_x(lax.rem(x + j, cols)), device_id_type=MESH)
    pl.semaphore_signal(barrier, 1, device_id=other_core, device_id_type=MESH)

    w_copies = [
        pltpu.make_async_copy(wg_hbm, wg, w_sem.at[0]),
        pltpu.make_async_copy(wu_hbm, wu, w_sem.at[1]),
        pltpu.make_async_copy(wd_hbm.at[:, :, my_cols], wd.at[core], w_sem.at[2]),
    ]
    for copy in w_copies:
        copy.start()

    r_k = [routing[k : k + 1, :] for k in range(top)]
    g_t = lax.div(r_k[0], epg)
    experts = epg * GROUPS
    earlier = (iota((tok, tok), 0) < iota((tok, tok), 1)).astype(BF16)
    e_io = iota((experts, tok), 0)
    named = jnp.zeros((experts, tok), F32)
    for k in range(top):
        named = named + (e_io == r_k[k]).astype(F32)
    rank = mm(named.astype(BF16), earlier)
    g_io = iota((16, tok), 0)
    in_group = (g_io == g_t).astype(F32)
    g_rank = mm(in_group.astype(BF16), earlier)
    pos = jnp.sum(in_group * g_rank, axis=0, keepdims=True).astype(I32)
    for k in range(top):
        rank_k = jnp.sum(jnp.where(e_io == r_k[k], rank, 0.0), axis=0, keepdims=True)
        sq_out[k : k + 1, :] = ((r_k[k] - g_t * epg) * cap + 1).astype(F32) + rank_k
        sq_out[top + k : top + k + 1, :] = prob[k : k + 1, :]
    wide = 2 * gmax
    wr = iota((GROUPS * wide, tok), 0)
    sel2 = (wr == g_t * wide + pos) | (wr == g_t * wide + gmax + pos)
    meta = lax.dot_general(
        sq_out[0 : 2 * top, :], sel2.astype(F32), (((1,), (1,)), ((), ())),
        preferred_element_type=F32, precision=lax.Precision.HIGHEST,
    )
    for g in range(GROUPS):
        meta_out[g] = meta[:, g * wide : (g + 1) * wide]
    place[...] = (iota((GROUPS * gmax, tok), 0) == g_t * gmax + pos).astype(BF16)

    floats = tokens[...].astype(F32)
    inv = lax.rsqrt(jnp.mean(floats * floats, axis=-1, keepdims=True) + EPS)
    normed = (tokens[:, my_cols].astype(F32) * inv * gain[:, my_cols]).astype(BF16)
    packed[...] = mm(place[...], normed).astype(BF16).reshape(packed.shape)

    pl.semaphore_wait(barrier, (lines - 1) + (cols - 1) + 1)

    def rel(a):
        return lax.rem(a + 2 * GROUPS, GROUPS)

    def meta_copy(j):
        zt = lax.rem(z + j, lines)
        gt = lax.div(zt, deep)
        return remote(
            meta_out.at[gt], meta_in.at[rel(grp - gt), o], m_send.at[j], m_recv.at[j], at_z(zt)
        )

    for j in range(1, lines):
        meta_copy(j).start()

    def chunk(d, s, q):
        return zbuf.at[d, lax.div(s, two), lax.rem(s, two), bits[q]]

    def first(t, row, i, d):
        gt = lax.rem(grp + t, GROUPS)
        return [
            remote(
                packed.at[gt, bits[q]], chunk(d, o, q), i_send.at[i, q], z_recv.at[d, o, q], at_z(row(gt))
            )
            for q in range(PARTS)
        ]

    opp = first(2, lambda gt: gt * deep + (deep - 1) * (1 - late), 2, 2)
    nxt = first(1, lambda gt: gt * deep, 1, 3)
    prv = first(3, lambda gt: gt * deep + deep - 1, 3, 1)
    own_up = first(0, lambda gt: lax.rem(z + 1, lines), 0, 0)
    own_dn = first(0, lambda gt: lax.rem(z + lines - 1, lines), 4, 0)

    def each(copies, what):
        def run_all():
            for copy in copies:
                getattr(copy, what)()

        return run_all

    wd_copy = remote(wd_hbm.at[:, :, peer_cols], wd.at[core], wd_send.at[0], wd_recv.at[0], other_core)
    wd_copy.start()
    zbuf[0, late, lax.rem(o, two)] = packed[grp]
    meta_in[0, o] = meta_out[grp]

    def onward(plus):
        zz = lax.rem(z + plus * 2 - 1 + lines, lines)
        more = ((plus == 1) & (o < deep - 1)) | ((plus == 0) & (o > 0))
        return zz, more

    def z_copy(d, s, plus, q):
        zz, more = onward(plus)
        here = chunk(d, s, q)
        return remote(here, here, z_send.at[d, s, q], z_recv.at[d, s, q], at_z(zz)), more

    def arrive(d, s, plus):
        for q in range(PARTS):
            copy, more = z_copy(d, s, plus, q)
            copy.wait_recv()
            pl.when(more)(copy.start)

    pair = two * gmax
    run = two * cap

    def x_to(src, dst, send, recv, d, h, j):
        xx = lax.rem(x + j, cols)
        return remote(src.at[d, h, xx], dst.at[d, h, x], send.at[d, h, j], recv.at[d, h, j], at_x(xx))

    def x_from(src, dst, send, recv, d, h, j):
        xx = lax.rem(x + cols - j, cols)
        return remote(src.at[d, h, xx], dst.at[d, h, xx], send.at[d, h, j], recv.at[d, h, j], at_x(xx))

    out_args = (xsend, rows.at[core], x_send, x_recv)
    back_args = (back_out, back_in, b_send, b_recv)
    x_order = [1, cols - 1] + list(range(2, cols - 1))

    def d_copy(d, h):
        return remote(rows.at[core, d, h], rows.at[core, d, h], d_send.at[d, h], d_recv.at[d, h], other_core)

    def d_arrival(d, h):
        return remote(rows.at[peer, d, h], rows.at[peer, d, h], d_send.at[d, h], d_recv.at[d, h], other_core)

    def select(d, h):
        lane = iota((2 * top, 2 * gmax), 1)
        info = jnp.where(lane < gmax, meta_in[d, two * h], meta_in[d, two * h + 1])
        zs = lax.div(iota((1, pair), 1), gmax)
        s_io = iota((pair, pair), 0)
        a = jnp.zeros((pair, pair), F32)
        w = jnp.zeros((pair, pair), F32)
        span = cols * loc * cap
        for k in range(top):
            v = info[k : k + 1, :].astype(I32) - 1 - span * o
            ok = (v >= 0) & (v < span)
            sid = jnp.where(ok, lax.div(v, cap) * run + zs * cap + lax.rem(v, cap), -1)
            hit = s_io == sid
            a = jnp.where(hit, 1.0, a)
            w = jnp.where(hit, info[top + k : top + k + 1, :], w)
        picked = mm(a.astype(BF16), zbuf[d, h].reshape(pair, half)).astype(BF16)
        xsend[d, h] = picked.reshape(cols, loc * run, half)
        for j in x_order:
            x_to(*out_args, d, h, j).start()
        rows[core, d, h, x] = xsend[d, h, x]
        hi = w.astype(BF16)
        mix_hi[d, h] = hi
        mix_lo[d, h] = (w - hi.astype(F32)).astype(BF16)

    def exchange(d, h):
        for j in x_order:
            x_from(*out_args, d, h, j).wait_recv()
        d_copy(d, h).start()

    m = cols * run

    def h_copy(d, h):
        return remote(hid.at[core, d, h], hid.at[core, d, h], h_send.at[d, h], h_recv.at[d, h], other_core)

    def h_arrival(d, h):
        return remote(hid.at[peer, d, h], hid.at[peer, d, h], h_send.at[d, h], h_recv.at[d, h], other_core)

    def gate_up(d, h):
        d_arrival(d, h).wait_recv()
        for e in range(loc):
            r = [rows[c, d, h, :, e * run : (e + 1) * run, :].reshape(m, half) for c in range(2)]
            ga = mm(r[0], wg[e, :half, :]) + mm(r[1], wg[e, half:, :])
            up = mm(r[0], wu[e, :half, :]) + mm(r[1], wu[e, half:, :])
            hid[core, d, h, e] = (ga / (1.0 + jnp.exp(-ga)) * up).astype(BF16)
        h_copy(d, h).start()

    def down(d, h):
        h_arrival(d, h).wait_recv()
        for e in range(loc):
            y = mm(hid[0, d, h, e], wd[0, e]) + mm(hid[1, d, h, e], wd[1, e])
            back_out[d, h, :, e * run : (e + 1) * run, :] = y.astype(BF16).reshape(cols, run, half)
        for j in x_order:
            x_to(*back_args, d, h, j).start()
        back_in[d, h, x] = back_out[d, h, x]

    def combine(d, h):
        for j in x_order:
            x_from(*back_args, d, h, j).wait_recv()
        res = back_in[d, h].reshape(pair, half)
        part[d, h] = mm_tn(mix_hi[d, h], res) + mm_tn(mix_lo[d, h], res)

    def landing(d, s, q, at, zz):
        return remote(
            psend.at[d, s, bits[q]], land.at[at, bits[q]], p_send.at[d, s, q], l_recv.at[at, q], at_z(zz)
        )

    def mine(d, s, q):
        at = pl.multiple_of(lax.rem(s, two) * gmax + q * bit, bit)
        return part[d, lax.div(s, two), pl.ds(at, bit), :]

    def send_back(d, s, plus):
        _, more = onward(plus)
        own = (d == 0).astype(I32)
        home = (1 - own) * (o == (deep - 1) * (1 - plus)).astype(I32)
        near = own * (s + plus * 2 - 1 == o).astype(I32)
        chain = d * deep + s
        at = home * (home_at + grp) + near * (side_at + 1 - plus) + (1 - home - near) * chain
        beside = lax.rem(z - (plus * 2 - 1) + lines, lines)
        zz = home * (lax.rem(grp + d, GROUPS) * deep + s) + (1 - home) * beside
        for q in range(PARTS):

            @pl.when(more)
            def _():
                landing(d, s, q, chain, z).wait_recv()
                psend[d, s, bits[q]] = (mine(d, s, q) + land[chain, bits[q]].astype(F32)).astype(BF16)

            @pl.when(jnp.logical_not(more))
            def _():
                psend[d, s, bits[q]] = mine(d, s, q).astype(BF16)

            landing(d, s, q, at, zz).start()

    def mirrored(kind, d, s):
        return (GROUPS - d) % GROUPS, (deep if kind in (ARRIVE, BACK) else 2) - 1 - s

    def pick(values):
        if len(set(values)) == 1:
            return jnp.int32(values[0])
        return sum(i * v for i, v in zip(in_row, values))

    def way(d, s, r):
        return {3: 1, 1: 0, 2: int(s >= two), 0: int(s < r)}[d]

    for n, (kind, d0, s0, d1, s1) in enumerate(PLAN):
        if kind == WAIT_META:
            for j in range(1, lines):
                meta_copy(j).wait_recv()
            continue
        if kind == WAIT_W:
            for copy in w_copies:
                copy.wait()
            remote(
                wd_hbm.at[:, :, my_cols], wd.at[peer], wd_send.at[0], wd_recv.at[0], other_core
            ).wait_recv()
            continue
        per_row = [(d0, s0), (d1, s1)]
        per_row += [mirrored(kind, *p) for p in per_row[::-1]]
        if kind == SEND:
            for t, copies in ((1, nxt), (2, opp), (3, prv)):
                flags = [int(p[0] == t) for p in per_row]
                if all(flags):
                    each(copies, "start")()
                elif any(flags):
                    pl.when(pick(flags) == 1)(each(copies, "start"))
            flags = [int(p[0] == 0) for p in per_row]
            if any(flags):
                pl.when((pick(flags) == 1) & (o < deep - 1))(each(own_up, "start"))
                pl.when((pick(flags) == 1) & (o > 0))(each(own_dn, "start"))
            continue
        d, s = pick([p[0] for p in per_row]), pick([p[1] for p in per_row])
        if kind in (ARRIVE, BACK):
            plus = pick([way(*p, r) for r, p in enumerate(per_row)])
            (arrive if kind == ARRIVE else send_back)(d, s, plus)
        else:
            {SELECT: select, EXCHANGE: exchange, GATE_UP: gate_up, DOWN: down, COMBINE: combine}[kind](d, s)

    own = jnp.concatenate([mine(0, o, q) for q in range(PARTS)], axis=0)

    @pl.when(o < deep - 1)
    def _():
        for q in range(PARTS):
            landing(0, o, q, side_at, z).wait_recv()

    @pl.when(o > 0)
    def _():
        for q in range(PARTS):
            landing(0, o, q, side_at + 1, z).wait_recv()

    own = own + jnp.where(o < deep - 1, land[side_at].astype(F32), 0.0)
    own = own + jnp.where(o > 0, land[side_at + 1].astype(F32), 0.0)
    for t in (1, 3, 2):
        gt = lax.rem(grp + t, GROUPS)
        for q in range(PARTS):
            landing(0, o, q, home_at + gt, z).wait_recv()
    ret[...] = land[home_at : home_at + GROUPS]
    ret[grp] = own.astype(BF16)
    mixed = mm_tn(place[...], ret[...].reshape(GROUPS * gmax, half))
    sq = jnp.zeros((tok, 128), F32)
    for i in range(half // 128):
        v = mixed[:, i * 128 : (i + 1) * 128]
        sq = sq + v * v
    sq_out[...] = sq
    q_copy = remote(sq_out, sq_in, q_send.at[0], q_recv.at[0], other_core)
    q_copy.start()
    q_copy.wait_recv()
    total = jnp.sum(sq_out[...] + sq_in[...], axis=1, keepdims=True)
    out_ref[...] = (mixed * lax.rsqrt(total / width + EPS) * out_gain[...]).astype(BF16)

    q_copy.wait_send()
    for j in range(1, lines):
        meta_copy(j).wait_send()
    each(opp + nxt + prv, "wait_send")()
    pl.when(o < deep - 1)(each(own_up, "wait_send"))
    pl.when(o > 0)(each(own_dn, "wait_send"))
    wd_copy.wait_send()

    def sent(d, s, plus):
        copies, more = [z_copy(d, s, plus, q)[0] for q in range(PARTS)], onward(plus)[1]
        pl.when(more)(each(copies, "wait_send"))
        for q in range(PARTS):
            landing(d, s, q, 0, z).wait_send()

    for s in range(deep):
        sent(2, s, s // two)
        sent(3, s, 1)
        sent(1, s, 0)
    for j in range(1, deep):
        s = lax.rem(o + j, deep)
        sent(0, s, (s < o).astype(I32))
    for d in range(GROUPS):
        for h in range(2):
            h_copy(d, h).wait_send()
            d_copy(d, h).wait_send()
            for j in range(1, cols):
                x_to(*out_args, d, h, j).wait_send()
                x_to(*back_args, d, h, j).wait_send()


def body(tokens, in_gain, routing, gate_prob, w_gate, w_up, w_down, out_gain):
    ep_count = lax.axis_size("ep")
    loc, width, ff = w_gate.shape
    tok, top = routing.shape
    half = out_gain.shape[0]
    epg = loc * ep_count // GROUPS
    cap = max(2, tok * top // (2 * epg))
    gmax = epg * cap // top
    side = math.isqrt(ep_count // GROUPS)
    lines = ep_count // side
    cols, deep = side, side
    two = deep // 2
    pair = two * gmax
    piece = loc * two * cap
    m = cols * two * cap
    cfg = (lines, side, tok, top, cap, gmax, half, width, epg)
    vmem = pl.BlockSpec(memory_space=pltpu.VMEM)
    anyw = pl.BlockSpec(memory_space=pl.ANY)
    dma = pltpu.SemaphoreType.DMA
    scratch = [
        pltpu.VMEM(w_gate.shape, BF16),
        pltpu.VMEM(w_up.shape, BF16),
        pltpu.VMEM((2, loc, ff, half), BF16),
        pltpu.VMEM((GROUPS * gmax, tok), BF16),
        pltpu.VMEM((GROUPS, 2 * top, 2 * gmax), F32),
        pltpu.VMEM((GROUPS, deep, 2 * top, 2 * gmax), F32),
        pltpu.VMEM((GROUPS, gmax, half), BF16),
        pltpu.VMEM((GROUPS, 2, two, gmax, half), BF16),
        pltpu.VMEM((GROUPS, 2, pair, pair), BF16),
        pltpu.VMEM((GROUPS, 2, pair, pair), BF16),
        pltpu.VMEM((GROUPS, 2, cols, piece, half), BF16),
        pltpu.VMEM((2, GROUPS, 2, cols, piece, half), BF16),
        pltpu.VMEM((2, GROUPS, 2, loc, m, ff), BF16),
        pltpu.VMEM((GROUPS, 2, cols, piece, half), BF16),
        pltpu.VMEM((GROUPS, 2, cols, piece, half), BF16),
        pltpu.VMEM((GROUPS, 2, pair, half), F32),
        pltpu.VMEM((GROUPS, deep, gmax, half), BF16),
        pltpu.VMEM((GROUPS * deep + GROUPS + 2, gmax, half), BF16),
        pltpu.VMEM((GROUPS, gmax, half), BF16),
        pltpu.VMEM((tok, 128), F32),
        pltpu.VMEM((tok, 128), F32),
        dma((3,)),
        dma((1,)),
        dma((1,)),
        dma((lines,)),
        dma((lines,)),
        dma((5, PARTS)),
        dma((GROUPS, deep, PARTS)),
        dma((GROUPS, deep, PARTS)),
        dma((GROUPS, 2, cols)),
        dma((GROUPS, 2, cols)),
        dma((GROUPS, 2)),
        dma((GROUPS, 2)),
        dma((GROUPS, 2)),
        dma((GROUPS, 2)),
        dma((GROUPS, 2, cols)),
        dma((GROUPS, 2, cols)),
        dma((GROUPS, deep, PARTS)),
        dma((GROUPS * deep + GROUPS + 2, PARTS)),
        dma((1,)),
        dma((1,)),
    ]
    return pl.pallas_call(
        functools.partial(kernel, cfg),
        out_shape=jax.ShapeDtypeStruct((tok, half), BF16),
        in_specs=[vmem] * 5 + [anyw] * 3,
        out_specs=vmem,
        scratch_shapes=scratch,
        compiler_params=pltpu.CompilerParams(
            collective_id=0, has_side_effects=True, vmem_limit_bytes=60 * 1024 * 1024
        ),
    )(
        routing.T, gate_prob.T, tokens, in_gain.reshape(1, width), out_gain.reshape(1, half),
        w_gate, w_up, w_down,
    )


def solution(mesh):
    placed = (
        P(("grp", "ep"), None),
        P(),
        P(("grp", "ep"), None),
        P(("grp", "ep"), None),
        P("ep", None, "tp"),
        P("ep", None, "tp"),
        P("ep", "tp", None),
        P("tp"),
    )
    return jax.shard_map(
        body, mesh=mesh, in_specs=placed, out_specs=P(("grp", "ep"), "tp"), check_vma=False
    )
```

```python
import functools
import math

import jax
import jax.numpy as jnp
from jax import lax
from jax.experimental import pallas as pl
from jax.experimental.pallas import tpu as pltpu
from jax.sharding import PartitionSpec as P

GROUPS = 4
EPS = 1e-06
MESH = pl.DeviceIdType.MESH
F32 = jnp.float32
BF16 = jnp.bfloat16
I32 = jnp.int32


def iota(shape, dim):
    return lax.broadcasted_iota(I32, shape, dim)


def mm(a, b):
    return jnp.dot(a, b, preferred_element_type=F32)


def mm_tn(a, b):
    return lax.dot_general(a, b, (((0,), (0,)), ((), ())), preferred_element_type=F32)


PARTS = 2
ARRIVE, BACK, SELECT, EXCHANGE, GATE_UP, DOWN, COMBINE, SEND, METAS, WAIT_W = range(10)

PLAN = (
    (SEND, 1, 0, 0, 0), (SEND, 0, 0, 3, 0), (SEND, 3, 0, 1, 0), (METAS, 0, 0, 0, 0),
    (ARRIVE, 3, 0, 0, 2), (ARRIVE, 0, 1, 0, 0), (SELECT, 0, 0, 0, 0), (ARRIVE, 3, 2, 3, 2),
    (ARRIVE, 0, 2, 3, 0), (ARRIVE, 3, 3, 0, 3), (SELECT, 3, 1, 0, 1), (SEND, 2, 0, 2, 0),
    (EXCHANGE, 0, 0, 0, 0), (WAIT_W, 0, 0, 0, 0), (GATE_UP, 0, 0, 0, 0), (ARRIVE, 0, 3, 3, 3),
    (SELECT, 0, 1, 3, 1), (DOWN, 0, 0, 0, 0), (ARRIVE, 3, 1, 1, 1), (ARRIVE, 2, 3, 3, 1),
    (ARRIVE, 2, 2, 1, 0), (EXCHANGE, 3, 1, 3, 1), (SELECT, 3, 0, 1, 0), (GATE_UP, 3, 1, 3, 1),
    (ARRIVE, 1, 1, 1, 3), (ARRIVE, 1, 0, 2, 3), (SELECT, 1, 0, 3, 0), (ARRIVE, 1, 3, 2, 2),
    (EXCHANGE, 0, 1, 1, 0), (EXCHANGE, 3, 0, 0, 1), (SELECT, 2, 1, 2, 1), (ARRIVE, 1, 2, 1, 2),
    (GATE_UP, 3, 0, 1, 0), (SELECT, 1, 1, 1, 1), (GATE_UP, 0, 1, 0, 1), (DOWN, 0, 1, 1, 0),
    (ARRIVE, 2, 0, 2, 1), (DOWN, 3, 1, 0, 1), (EXCHANGE, 1, 0, 2, 1), (ARRIVE, 2, 1, 2, 0),
    (COMBINE, 0, 1, 0, 1), (COMBINE, 0, 0, 1, 0), (EXCHANGE, 1, 1, 3, 0), (SELECT, 2, 0, 2, 0),
    (BACK, 0, 2, 0, 2), (EXCHANGE, 2, 1, 1, 1), (GATE_UP, 1, 0, 2, 1), (DOWN, 1, 0, 3, 1),
    (BACK, 0, 3, 0, 3), (GATE_UP, 1, 1, 1, 1), (EXCHANGE, 2, 0, 2, 0), (DOWN, 1, 1, 2, 1),
    (GATE_UP, 2, 0, 2, 0), (COMBINE, 1, 0, 3, 1), (DOWN, 2, 0, 2, 0), (BACK, 1, 0, 1, 0),
    (COMBINE, 3, 1, 0, 0), (GATE_UP, 2, 1, 3, 0), (BACK, 1, 1, 1, 1), (COMBINE, 2, 0, 2, 1),
    (BACK, 2, 1, 3, 3), (DOWN, 3, 0, 1, 1), (DOWN, 2, 1, 3, 0), (BACK, 2, 0, 0, 0),
    (COMBINE, 1, 1, 2, 0), (BACK, 1, 2, 2, 1), (BACK, 3, 3, 2, 0), (BACK, 1, 3, 2, 2),
    (COMBINE, 2, 1, 1, 1), (BACK, 2, 2, 3, 2), (BACK, 3, 2, 2, 3), (BACK, 2, 3, 1, 2),
    (BACK, 0, 1, 1, 3), (COMBINE, 3, 0, 3, 0), (BACK, 3, 1, 3, 1), (BACK, 3, 0, 3, 0),
)


def kernel(
    cfg, routing, prob, tokens, gain, out_gain, wg_hbm, wu_hbm, wd_hbm, out_ref,
    wg, wu, wd, place, meta_out, meta_in, packed, zbuf, mix_hi, mix_lo, xsend, rows, hid,
    back_out, back_in, part, psend, land, sq_out, sq_in,
    w_sem, wd_send, wd_recv, m_send, m_recv, i_send, z_send, z_recv, x_send, x_recv,
    d_send, d_recv, h_send, h_recv, b_send, b_recv, p_send, l_recv,
    q_send, q_recv,
):
    lines, side_len, tok, top, cap, gmax, half, width, epg = cfg
    cols, deep = side_len, side_len
    two = deep // 2
    bit = gmax // PARTS
    bits = [pl.ds(q * bit, bit) for q in range(PARTS)]
    home_at, side_at = GROUPS * deep, GROUPS * deep + GROUPS
    me = lax.axis_index("ep")
    core = lax.axis_index("tp")
    peer = 1 - core
    x, z = lax.rem(me, cols), lax.div(me, cols)
    grp, o = lax.div(z, deep), lax.rem(z, deep)
    late = lax.div(o, two)
    in_row = [(o == r).astype(I32) for r in range(deep)]
    loc = wg.shape[0]

    def at_z(zz):
        return {"ep": zz * cols + x}

    def at_x(xx):
        return {"ep": z * cols + xx}

    def remote(src, dst, s, r, dev):
        return pltpu.make_async_remote_copy(
            src_ref=src, dst_ref=dst, send_sem=s, recv_sem=r, device_id=dev, device_id_type=MESH
        )

    other_core = {"tp": peer}
    my_cols = pl.ds(pl.multiple_of(core * half, half), half)
    peer_cols = pl.ds(pl.multiple_of(peer * half, half), half)

    barrier = pltpu.get_barrier_semaphore()
    for j in range(1, lines):
        pl.semaphore_signal(barrier, 1, device_id=at_z(lax.rem(z + j, lines)), device_id_type=MESH)
    for j in range(1, cols):
        pl.semaphore_signal(barrier, 1, device_id=at_x(lax.rem(x + j, cols)), device_id_type=MESH)
    pl.semaphore_signal(barrier, 1, device_id=other_core, device_id_type=MESH)

    w_copies = [
        pltpu.make_async_copy(wg_hbm, wg, w_sem.at[0]),
        pltpu.make_async_copy(wu_hbm, wu, w_sem.at[1]),
        pltpu.make_async_copy(wd_hbm.at[:, :, my_cols], wd.at[core], w_sem.at[2]),
    ]
    for copy in w_copies:
        copy.start()

    r_k = [routing[k : k + 1, :] for k in range(top)]
    g_t = lax.div(r_k[0], epg)
    experts = epg * GROUPS
    earlier = (iota((tok, tok), 0) < iota((tok, tok), 1)).astype(BF16)
    e_io = iota((experts, tok), 0)
    named = jnp.zeros((experts, tok), F32)
    for k in range(top):
        named = named + (e_io == r_k[k]).astype(F32)
    rank = mm(named.astype(BF16), earlier)
    g_io = iota((16, tok), 0)
    in_group = (g_io == g_t).astype(F32)
    g_rank = mm(in_group.astype(BF16), earlier)
    pos = jnp.sum(in_group * g_rank, axis=0, keepdims=True).astype(I32)
    for k in range(top):
        rank_k = jnp.sum(jnp.where(e_io == r_k[k], rank, 0.0), axis=0, keepdims=True)
        sq_out[k : k + 1, :] = ((r_k[k] - g_t * epg) * cap + 1).astype(F32) + rank_k
        sq_out[top + k : top + k + 1, :] = prob[k : k + 1, :]
    wide = 2 * gmax
    wr = iota((GROUPS * wide, tok), 0)
    sel2 = (wr == g_t * wide + pos) | (wr == g_t * wide + gmax + pos)
    meta = lax.dot_general(
        sq_out[0 : 2 * top, :], sel2.astype(F32), (((1,), (1,)), ((), ())),
        preferred_element_type=F32, precision=lax.Precision.HIGHEST,
    )
    for g in range(GROUPS):
        meta_out[g] = meta[:, g * wide : (g + 1) * wide]
    place[...] = (iota((GROUPS * gmax, tok), 0) == g_t * gmax + pos).astype(BF16)

    floats = tokens[...].astype(F32)
    inv = lax.rsqrt(jnp.mean(floats * floats, axis=-1, keepdims=True) + EPS)
    normed = (tokens[:, my_cols].astype(F32) * inv * gain[:, my_cols]).astype(BF16)
    packed[...] = mm(place[...], normed).astype(BF16).reshape(packed.shape)

    pl.semaphore_wait(barrier, (lines - 1) + (cols - 1) + 1)

    def rel(a):
        return lax.rem(a + 2 * GROUPS, GROUPS)

    def meta_near(j):
        s = lax.rem(o + j, deep)
        return remote(
            meta_out.at[grp], meta_in.at[0, o], m_send.at[j], m_recv.at[0, o], at_z(grp * deep + s)
        )

    def meta_group(t):
        gt = lax.rem(grp + t, GROUPS)
        d = GROUPS - t
        return [
            remote(
                meta_out.at[gt], meta_in.at[d, o], m_send.at[t * deep + s], m_recv.at[d, o],
                at_z(gt * deep + s),
            )
            for s in range(deep)
        ]

    near_metas = [meta_near(j) for j in range(1, deep)]
    far_metas = [copy for t in (1, 3, 2) for copy in meta_group(t)]
    for copy in near_metas:
        copy.start()

    def chunk(d, s, q):
        return zbuf.at[d, lax.div(s, two), lax.rem(s, two), bits[q]]

    def first(t, row, i, d):
        gt = lax.rem(grp + t, GROUPS)
        return [
            remote(
                packed.at[gt, bits[q]], chunk(d, o, q), i_send.at[i, q], z_recv.at[d, o, q], at_z(row(gt))
            )
            for q in range(PARTS)
        ]

    opp = first(2, lambda gt: gt * deep + (deep - 1) * (1 - late), 2, 2)
    nxt = first(1, lambda gt: gt * deep, 1, 3)
    prv = first(3, lambda gt: gt * deep + deep - 1, 3, 1)
    own_up = first(0, lambda gt: lax.rem(z + 1, lines), 0, 0)
    own_dn = first(0, lambda gt: lax.rem(z + lines - 1, lines), 4, 0)

    def each(copies, what):
        def run_all():
            for copy in copies:
                getattr(copy, what)()

        return run_all

    wd_copy = remote(wd_hbm.at[:, :, peer_cols], wd.at[core], wd_send.at[0], wd_recv.at[0], other_core)
    wd_copy.start()
    zbuf[0, late, lax.rem(o, two)] = packed[grp]
    meta_in[0, o] = meta_out[grp]

    def onward(plus):
        zz = lax.rem(z + plus * 2 - 1 + lines, lines)
        more = ((plus == 1) & (o < deep - 1)) | ((plus == 0) & (o > 0))
        return zz, more

    def z_copy(d, s, plus, q):
        zz, more = onward(plus)
        here = chunk(d, s, q)
        return remote(here, here, z_send.at[d, s, q], z_recv.at[d, s, q], at_z(zz)), more

    def arrive(d, s, plus):
        for q in range(PARTS):
            copy, more = z_copy(d, s, plus, q)
            copy.wait_recv()
            pl.when(more)(copy.start)

    pair = two * gmax
    run = two * cap

    def x_to(src, dst, send, recv, d, h, j):
        xx = lax.rem(x + j, cols)
        return remote(src.at[d, h, xx], dst.at[d, h, x], send.at[d, h, j], recv.at[d, h, j], at_x(xx))

    def x_from(src, dst, send, recv, d, h, j):
        xx = lax.rem(x + cols - j, cols)
        return remote(src.at[d, h, xx], dst.at[d, h, xx], send.at[d, h, j], recv.at[d, h, j], at_x(xx))

    out_args = (xsend, rows.at[core], x_send, x_recv)
    back_args = (back_out, back_in, b_send, b_recv)
    x_order = [1, cols - 1] + list(range(2, cols - 1))

    def d_copy(d, h):
        return remote(rows.at[core, d, h], rows.at[core, d, h], d_send.at[d, h], d_recv.at[d, h], other_core)

    def d_arrival(d, h):
        return remote(rows.at[peer, d, h], rows.at[peer, d, h], d_send.at[d, h], d_recv.at[d, h], other_core)

    def select(d, h):
        for i in range(two):
            s = two * h + i
            pl.when((d != 0) | (s != o))(
                remote(meta_out.at[0], meta_in.at[d, s], m_send.at[0], m_recv.at[d, s], at_z(z)).wait_recv
            )
        lane = iota((2 * top, 2 * gmax), 1)
        info = jnp.where(lane < gmax, meta_in[d, two * h], meta_in[d, two * h + 1])
        zs = lax.div(iota((1, pair), 1), gmax)
        s_io = iota((pair, pair), 0)
        a = jnp.zeros((pair, pair), F32)
        w = jnp.zeros((pair, pair), F32)
        span = cols * loc * cap
        for k in range(top):
            v = info[k : k + 1, :].astype(I32) - 1 - span * o
            ok = (v >= 0) & (v < span)
            sid = jnp.where(ok, lax.div(v, cap) * run + zs * cap + lax.rem(v, cap), -1)
            hit = s_io == sid
            a = jnp.where(hit, 1.0, a)
            w = jnp.where(hit, info[top + k : top + k + 1, :], w)
        picked = mm(a.astype(BF16), zbuf[d, h].reshape(pair, half)).astype(BF16)
        xsend[d, h] = picked.reshape(cols, loc * run, half)
        for j in x_order:
            x_to(*out_args, d, h, j).start()
        rows[core, d, h, x] = xsend[d, h, x]
        hi = w.astype(BF16)
        mix_hi[d, h] = hi
        mix_lo[d, h] = (w - hi.astype(F32)).astype(BF16)

    def exchange(d, h):
        for j in x_order:
            x_from(*out_args, d, h, j).wait_recv()
        d_copy(d, h).start()

    m = cols * run

    def h_copy(d, h):
        return remote(hid.at[core, d, h], hid.at[core, d, h], h_send.at[d, h], h_recv.at[d, h], other_core)

    def h_arrival(d, h):
        return remote(hid.at[peer, d, h], hid.at[peer, d, h], h_send.at[d, h], h_recv.at[d, h], other_core)

    def gate_up(d, h):
        d_arrival(d, h).wait_recv()
        for e in range(loc):
            r = [rows[c, d, h, :, e * run : (e + 1) * run, :].reshape(m, half) for c in range(2)]
            ga = mm(r[0], wg[e, :half, :]) + mm(r[1], wg[e, half:, :])
            up = mm(r[0], wu[e, :half, :]) + mm(r[1], wu[e, half:, :])
            hid[core, d, h, e] = (ga / (1.0 + jnp.exp(-ga)) * up).astype(BF16)
        h_copy(d, h).start()

    def down(d, h):
        h_arrival(d, h).wait_recv()
        for e in range(loc):
            y = mm(hid[0, d, h, e], wd[0, e]) + mm(hid[1, d, h, e], wd[1, e])
            back_out[d, h, :, e * run : (e + 1) * run, :] = y.astype(BF16).reshape(cols, run, half)
        for j in x_order:
            x_to(*back_args, d, h, j).start()
        back_in[d, h, x] = back_out[d, h, x]

    def combine(d, h):
        for j in x_order:
            x_from(*back_args, d, h, j).wait_recv()
        res = back_in[d, h].reshape(pair, half)
        part[d, h] = mm_tn(mix_hi[d, h], res) + mm_tn(mix_lo[d, h], res)

    def landing(d, s, q, at, zz):
        return remote(
            psend.at[d, s, bits[q]], land.at[at, bits[q]], p_send.at[d, s, q], l_recv.at[at, q], at_z(zz)
        )

    def mine(d, s, q):
        at = pl.multiple_of(lax.rem(s, two) * gmax + q * bit, bit)
        return part[d, lax.div(s, two), pl.ds(at, bit), :]

    def send_back(d, s, plus):
        _, more = onward(plus)
        own = (d == 0).astype(I32)
        home = (1 - own) * (o == (deep - 1) * (1 - plus)).astype(I32)
        near = own * (s + plus * 2 - 1 == o).astype(I32)
        chain = d * deep + s
        at = home * (home_at + grp) + near * (side_at + 1 - plus) + (1 - home - near) * chain
        beside = lax.rem(z - (plus * 2 - 1) + lines, lines)
        zz = home * (lax.rem(grp + d, GROUPS) * deep + s) + (1 - home) * beside
        for q in range(PARTS):

            @pl.when(more)
            def _():
                landing(d, s, q, chain, z).wait_recv()
                psend[d, s, bits[q]] = (mine(d, s, q) + land[chain, bits[q]].astype(F32)).astype(BF16)

            @pl.when(jnp.logical_not(more))
            def _():
                psend[d, s, bits[q]] = mine(d, s, q).astype(BF16)

            landing(d, s, q, at, zz).start()

    def mirrored(kind, d, s):
        return (GROUPS - d) % GROUPS, (deep if kind in (ARRIVE, BACK) else 2) - 1 - s

    def pick(values):
        if len(set(values)) == 1:
            return jnp.int32(values[0])
        return sum(i * v for i, v in zip(in_row, values))

    def way(d, s, r):
        return {3: 1, 1: 0, 2: int(s >= two), 0: int(s < r)}[d]

    for n, (kind, d0, s0, d1, s1) in enumerate(PLAN):
        if kind == METAS:
            each(far_metas, "start")()
            continue
        if kind == WAIT_W:
            for copy in w_copies:
                copy.wait()
            remote(
                wd_hbm.at[:, :, my_cols], wd.at[peer], wd_send.at[0], wd_recv.at[0], other_core
            ).wait_recv()
            continue
        per_row = [(d0, s0), (d1, s1)]
        per_row += [mirrored(kind, *p) for p in per_row[::-1]]
        if kind == SEND:
            for t, copies in ((1, nxt), (2, opp), (3, prv)):
                flags = [int(p[0] == t) for p in per_row]
                if all(flags):
                    each(copies, "start")()
                elif any(flags):
                    pl.when(pick(flags) == 1)(each(copies, "start"))
            flags = [int(p[0] == 0) for p in per_row]
            if any(flags):
                pl.when((pick(flags) == 1) & (o < deep - 1))(each(own_up, "start"))
                pl.when((pick(flags) == 1) & (o > 0))(each(own_dn, "start"))
            continue
        d, s = pick([p[0] for p in per_row]), pick([p[1] for p in per_row])
        if kind in (ARRIVE, BACK):
            plus = pick([way(*p, r) for r, p in enumerate(per_row)])
            (arrive if kind == ARRIVE else send_back)(d, s, plus)
        else:
            {SELECT: select, EXCHANGE: exchange, GATE_UP: gate_up, DOWN: down, COMBINE: combine}[kind](d, s)

    own = jnp.concatenate([mine(0, o, q) for q in range(PARTS)], axis=0)

    @pl.when(o < deep - 1)
    def _():
        for q in range(PARTS):
            landing(0, o, q, side_at, z).wait_recv()

    @pl.when(o > 0)
    def _():
        for q in range(PARTS):
            landing(0, o, q, side_at + 1, z).wait_recv()

    own = own + jnp.where(o < deep - 1, land[side_at].astype(F32), 0.0)
    own = own + jnp.where(o > 0, land[side_at + 1].astype(F32), 0.0)
    for t in (1, 3, 2):
        gt = lax.rem(grp + t, GROUPS)
        for q in range(PARTS):
            landing(0, o, q, home_at + gt, z).wait_recv()
    land[home_at + grp] = own.astype(BF16)
    returned = land[home_at : home_at + GROUPS].reshape(GROUPS * gmax, half)
    mixed = mm_tn(place[...], returned)
    sq = jnp.zeros((tok, 128), F32)
    for i in range(half // 128):
        v = mixed[:, i * 128 : (i + 1) * 128]
        sq = sq + v * v
    sq_out[...] = sq
    q_copy = remote(sq_out, sq_in, q_send.at[0], q_recv.at[0], other_core)
    q_copy.start()
    q_copy.wait_recv()
    total = jnp.sum(sq_out[...] + sq_in[...], axis=1, keepdims=True)
    out_ref[...] = (mixed * lax.rsqrt(total / width + EPS) * out_gain[...]).astype(BF16)

    q_copy.wait_send()
    each(near_metas + far_metas, "wait_send")()
    each(opp + nxt + prv, "wait_send")()
    pl.when(o < deep - 1)(each(own_up, "wait_send"))
    pl.when(o > 0)(each(own_dn, "wait_send"))
    wd_copy.wait_send()

    def sent(d, s, plus):
        copies, more = [z_copy(d, s, plus, q)[0] for q in range(PARTS)], onward(plus)[1]
        pl.when(more)(each(copies, "wait_send"))
        for q in range(PARTS):
            landing(d, s, q, 0, z).wait_send()

    for s in range(deep):
        sent(2, s, s // two)
        sent(3, s, 1)
        sent(1, s, 0)
    for j in range(1, deep):
        s = lax.rem(o + j, deep)
        sent(0, s, (s < o).astype(I32))
    for d in range(GROUPS):
        for h in range(2):
            h_copy(d, h).wait_send()
            d_copy(d, h).wait_send()
            for j in range(1, cols):
                x_to(*out_args, d, h, j).wait_send()
                x_to(*back_args, d, h, j).wait_send()


def body(tokens, in_gain, routing, gate_prob, w_gate, w_up, w_down, out_gain):
    ep_count = lax.axis_size("ep")
    loc, width, ff = w_gate.shape
    tok, top = routing.shape
    half = out_gain.shape[0]
    epg = loc * ep_count // GROUPS
    cap = max(2, tok * top // (2 * epg))
    gmax = epg * cap // top
    side = math.isqrt(ep_count // GROUPS)
    lines = ep_count // side
    cols, deep = side, side
    two = deep // 2
    pair = two * gmax
    piece = loc * two * cap
    m = cols * two * cap
    cfg = (lines, side, tok, top, cap, gmax, half, width, epg)
    vmem = pl.BlockSpec(memory_space=pltpu.VMEM)
    anyw = pl.BlockSpec(memory_space=pl.ANY)
    dma = pltpu.SemaphoreType.DMA
    scratch = [
        pltpu.VMEM(w_gate.shape, BF16),
        pltpu.VMEM(w_up.shape, BF16),
        pltpu.VMEM((2, loc, ff, half), BF16),
        pltpu.VMEM((GROUPS * gmax, tok), BF16),
        pltpu.VMEM((GROUPS, 2 * top, 2 * gmax), F32),
        pltpu.VMEM((GROUPS, deep, 2 * top, 2 * gmax), F32),
        pltpu.VMEM((GROUPS, gmax, half), BF16),
        pltpu.VMEM((GROUPS, 2, two, gmax, half), BF16),
        pltpu.VMEM((GROUPS, 2, pair, pair), BF16),
        pltpu.VMEM((GROUPS, 2, pair, pair), BF16),
        pltpu.VMEM((GROUPS, 2, cols, piece, half), BF16),
        pltpu.VMEM((2, GROUPS, 2, cols, piece, half), BF16),
        pltpu.VMEM((2, GROUPS, 2, loc, m, ff), BF16),
        pltpu.VMEM((GROUPS, 2, cols, piece, half), BF16),
        pltpu.VMEM((GROUPS, 2, cols, piece, half), BF16),
        pltpu.VMEM((GROUPS, 2, pair, half), F32),
        pltpu.VMEM((GROUPS, deep, gmax, half), BF16),
        pltpu.VMEM((GROUPS * deep + GROUPS + 2, gmax, half), BF16),
        pltpu.VMEM((tok, 128), F32),
        pltpu.VMEM((tok, 128), F32),
        dma((3,)),
        dma((1,)),
        dma((1,)),
        dma((lines,)),
        dma((GROUPS, deep)),
        dma((5, PARTS)),
        dma((GROUPS, deep, PARTS)),
        dma((GROUPS, deep, PARTS)),
        dma((GROUPS, 2, cols)),
        dma((GROUPS, 2, cols)),
        dma((GROUPS, 2)),
        dma((GROUPS, 2)),
        dma((GROUPS, 2)),
        dma((GROUPS, 2)),
        dma((GROUPS, 2, cols)),
        dma((GROUPS, 2, cols)),
        dma((GROUPS, deep, PARTS)),
        dma((GROUPS * deep + GROUPS + 2, PARTS)),
        dma((1,)),
        dma((1,)),
    ]
    return pl.pallas_call(
        functools.partial(kernel, cfg),
        out_shape=jax.ShapeDtypeStruct((tok, half), BF16),
        in_specs=[vmem] * 5 + [anyw] * 3,
        out_specs=vmem,
        scratch_shapes=scratch,
        compiler_params=pltpu.CompilerParams(
            collective_id=0, has_side_effects=True, vmem_limit_bytes=60 * 1024 * 1024
        ),
    )(
        routing.T, gate_prob.T, tokens, in_gain.reshape(1, width), out_gain.reshape(1, half),
        w_gate, w_up, w_down,
    )


def solution(mesh):
    placed = (
        P(("grp", "ep"), None),
        P(),
        P(("grp", "ep"), None),
        P(("grp", "ep"), None),
        P("ep", None, "tp"),
        P("ep", None, "tp"),
        P("ep", "tp", None),
        P("tp"),
    )
    return jax.shard_map(
        body, mesh=mesh, in_specs=placed, out_specs=P(("grp", "ep"), "tp"), check_vma=False
    )
```

```python
import functools
import math

import jax
import jax.numpy as jnp
from jax import lax
from jax.experimental import pallas as pl
from jax.experimental.pallas import tpu as pltpu
from jax.sharding import PartitionSpec as P

GROUPS = 4
EPS = 1e-06
MESH = pl.DeviceIdType.MESH
F32 = jnp.float32
BF16 = jnp.bfloat16
I32 = jnp.int32


def iota(shape, dim):
    return lax.broadcasted_iota(I32, shape, dim)


def mm(a, b):
    return jnp.dot(a, b, preferred_element_type=F32)


def mm_tn(a, b):
    return lax.dot_general(a, b, (((0,), (0,)), ((), ())), preferred_element_type=F32)


PARTS = 4
ARRIVE, BACK, SELECT, EXCHANGE, GATE_UP, DOWN, COMBINE, SEND, METAS, WAIT_W = range(10)

PLAN = (
    (SEND, 1, 0, 0, 0), (SEND, 3, 0, 1, 0), (SEND, 0, 0, 3, 0), (METAS, 0, 0, 0, 0),
    (ARRIVE, 0, 1, 0, 0), (ARRIVE, 3, 0, 0, 2), (ARRIVE, 3, 3, 0, 3), (SELECT, 0, 0, 0, 0),
    (ARRIVE, 3, 2, 3, 2), (ARRIVE, 0, 2, 3, 3), (EXCHANGE, 0, 0, 0, 0), (SEND, 2, 0, 2, 0),
    (SELECT, 3, 1, 0, 1), (ARRIVE, 0, 3, 1, 1), (WAIT_W, 0, 0, 0, 0), (GATE_UP, 0, 0, 0, 0),
    (SELECT, 0, 1, 3, 1), (DOWN, 0, 0, 0, 0), (ARRIVE, 2, 3, 3, 0), (ARRIVE, 3, 1, 1, 0),
    (EXCHANGE, 0, 1, 0, 1), (ARRIVE, 1, 1, 2, 3), (ARRIVE, 2, 2, 3, 1), (SELECT, 2, 1, 1, 0),
    (ARRIVE, 1, 0, 1, 3), (GATE_UP, 0, 1, 0, 1), (DOWN, 0, 1, 0, 1), (ARRIVE, 1, 3, 2, 0),
    (ARRIVE, 2, 0, 2, 2), (SELECT, 1, 0, 2, 1), (ARRIVE, 2, 1, 2, 1), (SELECT, 2, 0, 2, 0),
    (ARRIVE, 1, 2, 1, 2), (EXCHANGE, 1, 0, 2, 0), (SELECT, 1, 1, 1, 1), (EXCHANGE, 2, 1, 1, 0),
    (EXCHANGE, 3, 1, 3, 1), (COMBINE, 0, 1, 0, 1), (COMBINE, 0, 0, 0, 0), (GATE_UP, 1, 0, 2, 0),
    (SELECT, 3, 0, 3, 0), (BACK, 0, 3, 0, 3), (GATE_UP, 3, 1, 1, 0), (EXCHANGE, 1, 1, 1, 1),
    (DOWN, 1, 0, 2, 0), (EXCHANGE, 2, 0, 2, 1), (GATE_UP, 1, 1, 3, 1), (EXCHANGE, 3, 0, 3, 0),
    (DOWN, 3, 1, 1, 0), (BACK, 0, 2, 0, 2), (GATE_UP, 2, 0, 1, 1), (DOWN, 2, 0, 3, 1),
    (COMBINE, 1, 0, 2, 0), (BACK, 1, 0, 0, 0), (GATE_UP, 2, 1, 2, 1), (COMBINE, 3, 1, 1, 0),
    (DOWN, 2, 1, 2, 1), (BACK, 1, 1, 1, 0), (GATE_UP, 3, 0, 3, 0), (COMBINE, 2, 0, 3, 1),
    (DOWN, 1, 1, 1, 1), (BACK, 2, 1, 2, 1), (BACK, 2, 0, 3, 3), (COMBINE, 1, 1, 2, 1),
    (BACK, 1, 3, 1, 1), (BACK, 1, 2, 2, 0), (BACK, 3, 3, 2, 2), (DOWN, 3, 0, 3, 0),
    (COMBINE, 2, 1, 1, 1), (BACK, 2, 2, 3, 2), (BACK, 3, 2, 2, 3), (COMBINE, 3, 0, 3, 0),
    (BACK, 2, 3, 1, 2), (BACK, 0, 1, 1, 3), (BACK, 3, 1, 3, 1), (BACK, 3, 0, 3, 0),
)


def kernel(
    cfg, routing, prob, tokens, gain, out_gain, wg_hbm, wu_hbm, wd_hbm, out_ref,
    wg, wu, wd, place, meta_out, meta_in, packed, zbuf, mix_hi, mix_lo, xsend, rows, hid,
    back_out, back_in, part, psend, land, sq_out, sq_in,
    w_sem, wd_send, wd_recv, m_send, m_recv, i_send, z_send, z_recv, x_send, x_recv,
    d_send, d_recv, h_send, h_recv, b_send, b_recv, p_send, l_recv,
    q_send, q_recv,
):
    lines, side_len, tok, top, cap, gmax, half, width, epg = cfg
    cols, deep = side_len, side_len
    two = deep // 2
    bit = gmax // PARTS
    bits = [pl.ds(q * bit, bit) for q in range(PARTS)]
    home_at, side_at = GROUPS * deep, GROUPS * deep + GROUPS
    me = lax.axis_index("ep")
    core = lax.axis_index("tp")
    peer = 1 - core
    x, z = lax.rem(me, cols), lax.div(me, cols)
    grp, o = lax.div(z, deep), lax.rem(z, deep)
    late = lax.div(o, two)
    in_row = [(o == r).astype(I32) for r in range(deep)]
    loc = wg.shape[0]

    def at_z(zz):
        return {"ep": zz * cols + x}

    def at_x(xx):
        return {"ep": z * cols + xx}

    def remote(src, dst, s, r, dev):
        return pltpu.make_async_remote_copy(
            src_ref=src, dst_ref=dst, send_sem=s, recv_sem=r, device_id=dev, device_id_type=MESH
        )

    other_core = {"tp": peer}
    my_cols = pl.ds(pl.multiple_of(core * half, half), half)
    peer_cols = pl.ds(pl.multiple_of(peer * half, half), half)

    barrier = pltpu.get_barrier_semaphore()
    for j in range(1, lines):
        pl.semaphore_signal(barrier, 1, device_id=at_z(lax.rem(z + j, lines)), device_id_type=MESH)
    for j in range(1, cols):
        pl.semaphore_signal(barrier, 1, device_id=at_x(lax.rem(x + j, cols)), device_id_type=MESH)
    pl.semaphore_signal(barrier, 1, device_id=other_core, device_id_type=MESH)

    w_copies = [
        pltpu.make_async_copy(wg_hbm, wg, w_sem.at[0]),
        pltpu.make_async_copy(wu_hbm, wu, w_sem.at[1]),
        pltpu.make_async_copy(wd_hbm.at[:, :, my_cols], wd.at[core], w_sem.at[2]),
    ]
    for copy in w_copies:
        copy.start()

    r_k = [routing[k : k + 1, :] for k in range(top)]
    g_t = lax.div(r_k[0], epg)
    experts = epg * GROUPS
    earlier = (iota((tok, tok), 0) < iota((tok, tok), 1)).astype(BF16)
    e_io = iota((experts, tok), 0)
    named = jnp.zeros((experts, tok), F32)
    for k in range(top):
        named = named + (e_io == r_k[k]).astype(F32)
    rank = mm(named.astype(BF16), earlier)
    g_io = iota((16, tok), 0)
    in_group = (g_io == g_t).astype(F32)
    g_rank = mm(in_group.astype(BF16), earlier)
    pos = jnp.sum(in_group * g_rank, axis=0, keepdims=True).astype(I32)
    for k in range(top):
        rank_k = jnp.sum(jnp.where(e_io == r_k[k], rank, 0.0), axis=0, keepdims=True)
        sq_out[k : k + 1, :] = ((r_k[k] - g_t * epg) * cap + 1).astype(F32) + rank_k
        sq_out[top + k : top + k + 1, :] = prob[k : k + 1, :]
    wide = 2 * gmax
    wr = iota((GROUPS * wide, tok), 0)
    sel2 = (wr == g_t * wide + pos) | (wr == g_t * wide + gmax + pos)
    meta = lax.dot_general(
        sq_out[0 : 2 * top, :], sel2.astype(F32), (((1,), (1,)), ((), ())),
        preferred_element_type=F32, precision=lax.Precision.HIGHEST,
    )
    for g in range(GROUPS):
        meta_out[g] = meta[:, g * wide : (g + 1) * wide]
    place[...] = (iota((GROUPS * gmax, tok), 0) == g_t * gmax + pos).astype(BF16)

    floats = tokens[...].astype(F32)
    inv = lax.rsqrt(jnp.mean(floats * floats, axis=-1, keepdims=True) + EPS)
    normed = (tokens[:, my_cols].astype(F32) * inv * gain[:, my_cols]).astype(BF16)
    packed[...] = mm(place[...], normed).astype(BF16).reshape(packed.shape)

    pl.semaphore_wait(barrier, (lines - 1) + (cols - 1) + 1)

    def rel(a):
        return lax.rem(a + 2 * GROUPS, GROUPS)

    def meta_near(j):
        s = lax.rem(o + j, deep)
        return remote(
            meta_out.at[grp], meta_in.at[0, o], m_send.at[j], m_recv.at[0, o], at_z(grp * deep + s)
        )

    def meta_group(t):
        gt = lax.rem(grp + t, GROUPS)
        d = GROUPS - t
        return [
            remote(
                meta_out.at[gt], meta_in.at[d, o], m_send.at[t * deep + s], m_recv.at[d, o],
                at_z(gt * deep + s),
            )
            for s in range(deep)
        ]

    near_metas = [meta_near(j) for j in range(1, deep)]
    far_metas = [copy for t in (1, 3, 2) for copy in meta_group(t)]
    for copy in near_metas:
        copy.start()

    def chunk(d, s, q):
        return zbuf.at[d, lax.div(s, two), lax.rem(s, two), bits[q]]

    def first(t, row, i, d):
        gt = lax.rem(grp + t, GROUPS)
        return [
            remote(
                packed.at[gt, bits[q]], chunk(d, o, q), i_send.at[i, q], z_recv.at[d, o, q], at_z(row(gt))
            )
            for q in range(PARTS)
        ]

    opp = first(2, lambda gt: gt * deep + (deep - 1) * (1 - late), 2, 2)
    nxt = first(1, lambda gt: gt * deep, 1, 3)
    prv = first(3, lambda gt: gt * deep + deep - 1, 3, 1)
    own_up = first(0, lambda gt: lax.rem(z + 1, lines), 0, 0)
    own_dn = first(0, lambda gt: lax.rem(z + lines - 1, lines), 4, 0)

    def each(copies, what):
        def run_all():
            for copy in copies:
                getattr(copy, what)()

        return run_all

    wd_copy = remote(wd_hbm.at[:, :, peer_cols], wd.at[core], wd_send.at[0], wd_recv.at[0], other_core)
    wd_copy.start()
    zbuf[0, late, lax.rem(o, two)] = packed[grp]
    meta_in[0, o] = meta_out[grp]

    def onward(plus):
        zz = lax.rem(z + plus * 2 - 1 + lines, lines)
        more = ((plus == 1) & (o < deep - 1)) | ((plus == 0) & (o > 0))
        return zz, more

    def z_copy(d, s, plus, q):
        zz, more = onward(plus)
        here = chunk(d, s, q)
        return remote(here, here, z_send.at[d, s, q], z_recv.at[d, s, q], at_z(zz)), more

    def arrive(d, s, plus):
        for q in range(PARTS):
            copy, more = z_copy(d, s, plus, q)
            copy.wait_recv()
            pl.when(more)(copy.start)

    pair = two * gmax
    run = two * cap

    def x_to(src, dst, send, recv, d, h, j):
        xx = lax.rem(x + j, cols)
        return remote(src.at[d, h, xx], dst.at[d, h, x], send.at[d, h, j], recv.at[d, h, j], at_x(xx))

    def x_from(src, dst, send, recv, d, h, j):
        xx = lax.rem(x + cols - j, cols)
        return remote(src.at[d, h, xx], dst.at[d, h, xx], send.at[d, h, j], recv.at[d, h, j], at_x(xx))

    out_args = (xsend, rows.at[core], x_send, x_recv)
    back_args = (back_out, back_in, b_send, b_recv)
    x_order = [1, cols - 1] + list(range(2, cols - 1))

    def d_copy(d, h):
        return remote(rows.at[core, d, h], rows.at[core, d, h], d_send.at[d, h], d_recv.at[d, h], other_core)

    def d_arrival(d, h):
        return remote(rows.at[peer, d, h], rows.at[peer, d, h], d_send.at[d, h], d_recv.at[d, h], other_core)

    def select(d, h):
        for i in range(two):
            s = two * h + i
            pl.when((d != 0) | (s != o))(
                remote(meta_out.at[0], meta_in.at[d, s], m_send.at[0], m_recv.at[d, s], at_z(z)).wait_recv
            )
        lane = iota((2 * top, 2 * gmax), 1)
        info = jnp.where(lane < gmax, meta_in[d, two * h], meta_in[d, two * h + 1])
        zs = lax.div(iota((1, pair), 1), gmax)
        s_io = iota((pair, pair), 0)
        a = jnp.zeros((pair, pair), F32)
        w = jnp.zeros((pair, pair), F32)
        span = cols * loc * cap
        for k in range(top):
            v = info[k : k + 1, :].astype(I32) - 1 - span * o
            ok = (v >= 0) & (v < span)
            sid = jnp.where(ok, lax.div(v, cap) * run + zs * cap + lax.rem(v, cap), -1)
            hit = s_io == sid
            a = jnp.where(hit, 1.0, a)
            w = jnp.where(hit, info[top + k : top + k + 1, :], w)
        picked = mm(a.astype(BF16), zbuf[d, h].reshape(pair, half)).astype(BF16)
        xsend[d, h] = picked.reshape(cols, loc * run, half)
        for j in x_order:
            x_to(*out_args, d, h, j).start()
        rows[core, d, h, x] = xsend[d, h, x]
        hi = w.astype(BF16)
        mix_hi[d, h] = hi
        mix_lo[d, h] = (w - hi.astype(F32)).astype(BF16)

    def exchange(d, h):
        for j in x_order:
            x_from(*out_args, d, h, j).wait_recv()
        d_copy(d, h).start()

    m = cols * run

    def h_copy(d, h):
        return remote(hid.at[core, d, h], hid.at[core, d, h], h_send.at[d, h], h_recv.at[d, h], other_core)

    def h_arrival(d, h):
        return remote(hid.at[peer, d, h], hid.at[peer, d, h], h_send.at[d, h], h_recv.at[d, h], other_core)

    def gate_up(d, h):
        d_arrival(d, h).wait_recv()
        for e in range(loc):
            r = [rows[c, d, h, :, e * run : (e + 1) * run, :].reshape(m, half) for c in range(2)]
            ga = mm(r[0], wg[e, :half, :]) + mm(r[1], wg[e, half:, :])
            up = mm(r[0], wu[e, :half, :]) + mm(r[1], wu[e, half:, :])
            hid[core, d, h, e] = (ga / (1.0 + jnp.exp(-ga)) * up).astype(BF16)
        h_copy(d, h).start()

    def down(d, h):
        h_arrival(d, h).wait_recv()
        for e in range(loc):
            y = mm(hid[0, d, h, e], wd[0, e]) + mm(hid[1, d, h, e], wd[1, e])
            back_out[d, h, :, e * run : (e + 1) * run, :] = y.astype(BF16).reshape(cols, run, half)
        for j in x_order:
            x_to(*back_args, d, h, j).start()
        back_in[d, h, x] = back_out[d, h, x]

    def combine(d, h):
        for j in x_order:
            x_from(*back_args, d, h, j).wait_recv()
        res = back_in[d, h].reshape(pair, half)
        part[d, h] = mm_tn(mix_hi[d, h], res) + mm_tn(mix_lo[d, h], res)

    def landing(d, s, q, at, zz):
        return remote(
            psend.at[d, s, bits[q]], land.at[at, bits[q]], p_send.at[d, s, q], l_recv.at[at, q], at_z(zz)
        )

    def mine(d, s, q):
        at = pl.multiple_of(lax.rem(s, two) * gmax + q * bit, bit)
        return part[d, lax.div(s, two), pl.ds(at, bit), :]

    def send_back(d, s, plus):
        _, more = onward(plus)
        own = (d == 0).astype(I32)
        home = (1 - own) * (o == (deep - 1) * (1 - plus)).astype(I32)
        near = own * (s + plus * 2 - 1 == o).astype(I32)
        chain = d * deep + s
        at = home * (home_at + grp) + near * (side_at + 1 - plus) + (1 - home - near) * chain
        beside = lax.rem(z - (plus * 2 - 1) + lines, lines)
        zz = home * (lax.rem(grp + d, GROUPS) * deep + s) + (1 - home) * beside
        for q in range(PARTS):

            @pl.when(more)
            def _():
                landing(d, s, q, chain, z).wait_recv()
                psend[d, s, bits[q]] = (mine(d, s, q) + land[chain, bits[q]].astype(F32)).astype(BF16)

            @pl.when(jnp.logical_not(more))
            def _():
                psend[d, s, bits[q]] = mine(d, s, q).astype(BF16)

            landing(d, s, q, at, zz).start()

    def mirrored(kind, d, s):
        return (GROUPS - d) % GROUPS, (deep if kind in (ARRIVE, BACK) else 2) - 1 - s

    def pick(values):
        if len(set(values)) == 1:
            return jnp.int32(values[0])
        return sum(i * v for i, v in zip(in_row, values))

    def way(d, s, r):
        return {3: 1, 1: 0, 2: int(s >= two), 0: int(s < r)}[d]

    for n, (kind, d0, s0, d1, s1) in enumerate(PLAN):
        if kind == METAS:
            each(far_metas, "start")()
            continue
        if kind == WAIT_W:
            for copy in w_copies:
                copy.wait()
            remote(
                wd_hbm.at[:, :, my_cols], wd.at[peer], wd_send.at[0], wd_recv.at[0], other_core
            ).wait_recv()
            continue
        per_row = [(d0, s0), (d1, s1)]
        per_row += [mirrored(kind, *p) for p in per_row[::-1]]
        if kind == SEND:
            for t, copies in ((1, nxt), (2, opp), (3, prv)):
                flags = [int(p[0] == t) for p in per_row]
                if all(flags):
                    each(copies, "start")()
                elif any(flags):
                    pl.when(pick(flags) == 1)(each(copies, "start"))
            flags = [int(p[0] == 0) for p in per_row]
            if any(flags):
                pl.when((pick(flags) == 1) & (o < deep - 1))(each(own_up, "start"))
                pl.when((pick(flags) == 1) & (o > 0))(each(own_dn, "start"))
            continue
        d, s = pick([p[0] for p in per_row]), pick([p[1] for p in per_row])
        if kind in (ARRIVE, BACK):
            plus = pick([way(*p, r) for r, p in enumerate(per_row)])
            (arrive if kind == ARRIVE else send_back)(d, s, plus)
        else:
            {SELECT: select, EXCHANGE: exchange, GATE_UP: gate_up, DOWN: down, COMBINE: combine}[kind](d, s)

    own = jnp.concatenate([mine(0, o, q) for q in range(PARTS)], axis=0)

    @pl.when(o < deep - 1)
    def _():
        for q in range(PARTS):
            landing(0, o, q, side_at, z).wait_recv()

    @pl.when(o > 0)
    def _():
        for q in range(PARTS):
            landing(0, o, q, side_at + 1, z).wait_recv()

    own = own + jnp.where(o < deep - 1, land[side_at].astype(F32), 0.0)
    own = own + jnp.where(o > 0, land[side_at + 1].astype(F32), 0.0)
    for t in (1, 3, 2):
        gt = lax.rem(grp + t, GROUPS)
        for q in range(PARTS):
            landing(0, o, q, home_at + gt, z).wait_recv()
    land[home_at + grp] = own.astype(BF16)
    returned = land[home_at : home_at + GROUPS].reshape(GROUPS * gmax, half)
    mixed = mm_tn(place[...], returned)
    sq = jnp.zeros((tok, 128), F32)
    for i in range(half // 128):
        v = mixed[:, i * 128 : (i + 1) * 128]
        sq = sq + v * v
    sq_out[...] = sq
    q_copy = remote(sq_out, sq_in, q_send.at[0], q_recv.at[0], other_core)
    q_copy.start()
    q_copy.wait_recv()
    total = jnp.sum(sq_out[...] + sq_in[...], axis=1, keepdims=True)
    out_ref[...] = (mixed * lax.rsqrt(total / width + EPS) * out_gain[...]).astype(BF16)

    q_copy.wait_send()
    each(near_metas + far_metas, "wait_send")()
    each(opp + nxt + prv, "wait_send")()
    pl.when(o < deep - 1)(each(own_up, "wait_send"))
    pl.when(o > 0)(each(own_dn, "wait_send"))
    wd_copy.wait_send()

    def sent(d, s, plus):
        copies, more = [z_copy(d, s, plus, q)[0] for q in range(PARTS)], onward(plus)[1]
        pl.when(more)(each(copies, "wait_send"))
        for q in range(PARTS):
            landing(d, s, q, 0, z).wait_send()

    for s in range(deep):
        sent(2, s, s // two)
        sent(3, s, 1)
        sent(1, s, 0)
    for j in range(1, deep):
        s = lax.rem(o + j, deep)
        sent(0, s, (s < o).astype(I32))
    for d in range(GROUPS):
        for h in range(2):
            h_copy(d, h).wait_send()
            d_copy(d, h).wait_send()
            for j in range(1, cols):
                x_to(*out_args, d, h, j).wait_send()
                x_to(*back_args, d, h, j).wait_send()


def body(tokens, in_gain, routing, gate_prob, w_gate, w_up, w_down, out_gain):
    ep_count = lax.axis_size("ep")
    loc, width, ff = w_gate.shape
    tok, top = routing.shape
    half = out_gain.shape[0]
    epg = loc * ep_count // GROUPS
    cap = max(2, tok * top // (2 * epg))
    gmax = epg * cap // top
    side = math.isqrt(ep_count // GROUPS)
    lines = ep_count // side
    cols, deep = side, side
    two = deep // 2
    pair = two * gmax
    piece = loc * two * cap
    m = cols * two * cap
    cfg = (lines, side, tok, top, cap, gmax, half, width, epg)
    vmem = pl.BlockSpec(memory_space=pltpu.VMEM)
    anyw = pl.BlockSpec(memory_space=pl.ANY)
    dma = pltpu.SemaphoreType.DMA
    scratch = [
        pltpu.VMEM(w_gate.shape, BF16),
        pltpu.VMEM(w_up.shape, BF16),
        pltpu.VMEM((2, loc, ff, half), BF16),
        pltpu.VMEM((GROUPS * gmax, tok), BF16),
        pltpu.VMEM((GROUPS, 2 * top, 2 * gmax), F32),
        pltpu.VMEM((GROUPS, deep, 2 * top, 2 * gmax), F32),
        pltpu.VMEM((GROUPS, gmax, half), BF16),
        pltpu.VMEM((GROUPS, 2, two, gmax, half), BF16),
        pltpu.VMEM((GROUPS, 2, pair, pair), BF16),
        pltpu.VMEM((GROUPS, 2, pair, pair), BF16),
        pltpu.VMEM((GROUPS, 2, cols, piece, half), BF16),
        pltpu.VMEM((2, GROUPS, 2, cols, piece, half), BF16),
        pltpu.VMEM((2, GROUPS, 2, loc, m, ff), BF16),
        pltpu.VMEM((GROUPS, 2, cols, piece, half), BF16),
        pltpu.VMEM((GROUPS, 2, cols, piece, half), BF16),
        pltpu.VMEM((GROUPS, 2, pair, half), F32),
        pltpu.VMEM((GROUPS, deep, gmax, half), BF16),
        pltpu.VMEM((GROUPS * deep + GROUPS + 2, gmax, half), BF16),
        pltpu.VMEM((tok, 128), F32),
        pltpu.VMEM((tok, 128), F32),
        dma((3,)),
        dma((1,)),
        dma((1,)),
        dma((lines,)),
        dma((GROUPS, deep)),
        dma((5, PARTS)),
        dma((GROUPS, deep, PARTS)),
        dma((GROUPS, deep, PARTS)),
        dma((GROUPS, 2, cols)),
        dma((GROUPS, 2, cols)),
        dma((GROUPS, 2)),
        dma((GROUPS, 2)),
        dma((GROUPS, 2)),
        dma((GROUPS, 2)),
        dma((GROUPS, 2, cols)),
        dma((GROUPS, 2, cols)),
        dma((GROUPS, deep, PARTS)),
        dma((GROUPS * deep + GROUPS + 2, PARTS)),
        dma((1,)),
        dma((1,)),
    ]
    return pl.pallas_call(
        functools.partial(kernel, cfg),
        out_shape=jax.ShapeDtypeStruct((tok, half), BF16),
        in_specs=[vmem] * 5 + [anyw] * 3,
        out_specs=vmem,
        scratch_shapes=scratch,
        compiler_params=pltpu.CompilerParams(
            collective_id=0, has_side_effects=True, vmem_limit_bytes=60 * 1024 * 1024
        ),
    )(
        routing.T, gate_prob.T, tokens, in_gain.reshape(1, width), out_gain.reshape(1, half),
        w_gate, w_up, w_down,
    )


def solution(mesh):
    placed = (
        P(("grp", "ep"), None),
        P(),
        P(("grp", "ep"), None),
        P(("grp", "ep"), None),
        P("ep", None, "tp"),
        P("ep", None, "tp"),
        P("ep", "tp", None),
        P("tp"),
    )
    return jax.shard_map(
        body, mesh=mesh, in_specs=placed, out_specs=P(("grp", "ep"), "tp"), check_vma=False
    )
```

```python
import functools
import math

import jax
import jax.numpy as jnp
from jax import lax
from jax.experimental import pallas as pl
from jax.experimental.pallas import tpu as pltpu
from jax.sharding import PartitionSpec as P

GROUPS = 4
EPS = 1e-06
MESH = pl.DeviceIdType.MESH
F32 = jnp.float32
BF16 = jnp.bfloat16
I32 = jnp.int32


def iota(shape, dim):
    return lax.broadcasted_iota(I32, shape, dim)


def mm(a, b):
    return jnp.dot(a, b, preferred_element_type=F32)


def mm_tn(a, b):
    return lax.dot_general(a, b, (((0,), (0,)), ((), ())), preferred_element_type=F32)


PARTS = 2
ARRIVE, BACK, SELECT, EXCHANGE, GATE_UP, DOWN, COMBINE, SEND, METAS, WAIT_W = range(10)

PLAN = (
    (SEND, 1, 0, 0, 0), (SEND, 3, 0, 1, 0), (SEND, 0, 0, 3, 0), (METAS, 0, 0, 0, 0),
    (ARRIVE, 0, 1, 0, 2), (ARRIVE, 3, 3, 0, 0), (SELECT, 0, 0, 0, 0), (ARRIVE, 3, 0, 0, 3),
    (ARRIVE, 3, 2, 3, 0), (EXCHANGE, 0, 0, 0, 0), (SELECT, 3, 1, 0, 1), (SEND, 2, 0, 2, 0),
    (ARRIVE, 0, 2, 3, 3), (WAIT_W, 0, 0, 0, 0), (GATE_UP, 0, 0, 0, 0), (DOWN, 0, 0, 0, 0),
    (ARRIVE, 0, 3, 3, 2), (ARRIVE, 2, 3, 1, 0), (SELECT, 0, 1, 3, 1), (ARRIVE, 3, 1, 2, 3),
    (EXCHANGE, 0, 1, 0, 1), (COMBINE, 0, 0, 0, 0), (ARRIVE, 2, 2, 1, 1), (SELECT, 2, 1, 1, 0),
    (ARRIVE, 1, 0, 3, 1), (ARRIVE, 1, 1, 1, 3), (GATE_UP, 0, 1, 0, 1), (DOWN, 0, 1, 0, 1),
    (EXCHANGE, 2, 1, 3, 1), (ARRIVE, 1, 3, 2, 0), (ARRIVE, 2, 0, 2, 2), (SELECT, 1, 0, 3, 0),
    (ARRIVE, 2, 1, 2, 1), (EXCHANGE, 3, 1, 1, 0), (SELECT, 2, 0, 2, 0), (ARRIVE, 1, 2, 1, 2),
    (EXCHANGE, 1, 0, 2, 0), (SELECT, 1, 1, 2, 1), (GATE_UP, 3, 1, 1, 0), (EXCHANGE, 2, 0, 3, 0),
    (SELECT, 3, 0, 1, 1), (COMBINE, 0, 1, 0, 1), (BACK, 0, 3, 0, 3), (GATE_UP, 1, 0, 2, 0),
    (DOWN, 1, 0, 1, 0), (GATE_UP, 2, 1, 3, 1), (EXCHANGE, 1, 1, 1, 1), (BACK, 0, 2, 0, 2),
    (EXCHANGE, 3, 0, 2, 1), (DOWN, 3, 1, 2, 0), (GATE_UP, 2, 0, 2, 1), (DOWN, 2, 0, 3, 1),
    (COMBINE, 1, 0, 1, 0), (BACK, 1, 0, 1, 0), (BACK, 1, 1, 0, 0), (GATE_UP, 1, 1, 3, 0),
    (GATE_UP, 3, 0, 1, 1), (DOWN, 1, 1, 2, 1), (COMBINE, 2, 0, 2, 0), (BACK, 2, 1, 1, 1),
    (COMBINE, 1, 1, 3, 1), (BACK, 2, 0, 2, 1), (BACK, 1, 2, 3, 3), (DOWN, 2, 1, 1, 1),
    (COMBINE, 3, 1, 2, 1), (BACK, 1, 3, 2, 0), (BACK, 3, 3, 2, 2), (DOWN, 3, 0, 3, 0),
    (COMBINE, 2, 1, 1, 1), (BACK, 2, 2, 3, 2), (COMBINE, 3, 0, 3, 0), (BACK, 3, 2, 1, 2),
    (BACK, 2, 3, 1, 3), (BACK, 0, 1, 2, 3), (BACK, 3, 1, 3, 1), (BACK, 3, 0, 3, 0),
)


def kernel(
    cfg, routing, prob, tokens, gain, out_gain, wg_hbm, wu_hbm, wd_hbm, out_ref,
    wg, wu, wd, place, meta_out, meta_in, packed, zbuf, mix_hi, mix_lo, xsend, rows, hid,
    back_out, back_in, part, psend, land, sq_out, sq_in,
    w_sem, wd_send, wd_recv, m_send, m_recv, i_send, z_send, z_recv, x_send, x_recv,
    d_send, d_recv, h_send, h_recv, b_send, b_recv, p_send, l_recv,
    q_send, q_recv,
):
    lines, side_len, tok, top, cap, gmax, half, width, epg = cfg
    cols, deep = side_len, side_len
    two = deep // 2
    bit = gmax // PARTS
    bits = [pl.ds(q * bit, bit) for q in range(PARTS)]
    home_at, side_at = GROUPS * deep, GROUPS * deep + GROUPS
    me = lax.axis_index("ep")
    core = lax.axis_index("tp")
    peer = 1 - core
    x, z = lax.rem(me, cols), lax.div(me, cols)
    grp, o = lax.div(z, deep), lax.rem(z, deep)
    late = lax.div(o, two)
    in_row = [(o == r).astype(I32) for r in range(deep)]
    loc = wg.shape[0]

    def at_z(zz):
        return {"ep": zz * cols + x}

    def at_x(xx):
        return {"ep": z * cols + xx}

    def remote(src, dst, s, r, dev):
        return pltpu.make_async_remote_copy(
            src_ref=src, dst_ref=dst, send_sem=s, recv_sem=r, device_id=dev, device_id_type=MESH
        )

    other_core = {"tp": peer}
    my_cols = pl.ds(pl.multiple_of(core * half, half), half)
    peer_cols = pl.ds(pl.multiple_of(peer * half, half), half)

    barrier = pltpu.get_barrier_semaphore()
    for j in range(1, lines):
        pl.semaphore_signal(barrier, 1, device_id=at_z(lax.rem(z + j, lines)), device_id_type=MESH)
    for j in range(1, cols):
        pl.semaphore_signal(barrier, 1, device_id=at_x(lax.rem(x + j, cols)), device_id_type=MESH)
    pl.semaphore_signal(barrier, 1, device_id=other_core, device_id_type=MESH)

    w_copies = [
        pltpu.make_async_copy(wg_hbm, wg, w_sem.at[0]),
        pltpu.make_async_copy(wu_hbm, wu, w_sem.at[1]),
        pltpu.make_async_copy(wd_hbm.at[:, :, my_cols], wd.at[core], w_sem.at[2]),
    ]
    for copy in w_copies:
        copy.start()

    r_k = [routing[k : k + 1, :] for k in range(top)]
    g_t = lax.div(r_k[0], epg)
    experts = epg * GROUPS
    earlier = (iota((tok, tok), 0) < iota((tok, tok), 1)).astype(BF16)
    e_io = iota((experts, tok), 0)
    named = jnp.zeros((experts, tok), F32)
    for k in range(top):
        named = named + (e_io == r_k[k]).astype(F32)
    rank = mm(named.astype(BF16), earlier)
    g_io = iota((16, tok), 0)
    in_group = (g_io == g_t).astype(F32)
    g_rank = mm(in_group.astype(BF16), earlier)
    pos = jnp.sum(in_group * g_rank, axis=0, keepdims=True).astype(I32)
    for k in range(top):
        rank_k = jnp.sum(jnp.where(e_io == r_k[k], rank, 0.0), axis=0, keepdims=True)
        sq_out[k : k + 1, :] = ((r_k[k] - g_t * epg) * cap + 1).astype(F32) + rank_k
        sq_out[top + k : top + k + 1, :] = prob[k : k + 1, :]
    wide = 2 * gmax
    wr = iota((GROUPS * wide, tok), 0)
    sel2 = (wr == g_t * wide + pos) | (wr == g_t * wide + gmax + pos)
    meta = lax.dot_general(
        sq_out[0 : 2 * top, :], sel2.astype(F32), (((1,), (1,)), ((), ())),
        preferred_element_type=F32, precision=lax.Precision.HIGHEST,
    )
    for g in range(GROUPS):
        meta_out[g] = meta[:, g * wide : (g + 1) * wide]
    place[...] = (iota((GROUPS * gmax, tok), 0) == g_t * gmax + pos).astype(BF16)

    floats = tokens[...].astype(F32)
    inv = lax.rsqrt(jnp.mean(floats * floats, axis=-1, keepdims=True) + EPS)
    normed = (tokens[:, my_cols].astype(F32) * inv * gain[:, my_cols]).astype(BF16)
    packed[...] = mm(place[...], normed).astype(BF16).reshape(packed.shape)

    pl.semaphore_wait(barrier, (lines - 1) + (cols - 1) + 1)

    def rel(a):
        return lax.rem(a + 2 * GROUPS, GROUPS)

    def meta_near(j):
        s = lax.rem(o + j, deep)
        return remote(
            meta_out.at[grp], meta_in.at[0, o], m_send.at[j], m_recv.at[0, o], at_z(grp * deep + s)
        )

    def meta_group(t):
        gt = lax.rem(grp + t, GROUPS)
        d = GROUPS - t
        return [
            remote(
                meta_out.at[gt], meta_in.at[d, o], m_send.at[t * deep + s], m_recv.at[d, o],
                at_z(gt * deep + s),
            )
            for s in range(deep)
        ]

    near_metas = [meta_near(j) for j in range(1, deep)]
    far_metas = [copy for t in (1, 3, 2) for copy in meta_group(t)]
    for copy in near_metas:
        copy.start()

    def chunk(d, s, q):
        return zbuf.at[d, lax.div(s, two), lax.rem(s, two), bits[q]]

    def first(t, row, i, d):
        gt = lax.rem(grp + t, GROUPS)
        return [
            remote(
                packed.at[gt, bits[q]], chunk(d, o, q), i_send.at[i, q], z_recv.at[d, o, q], at_z(row(gt))
            )
            for q in range(PARTS)
        ]

    opp = first(2, lambda gt: gt * deep + (deep - 1) * (1 - late), 2, 2)
    nxt = first(1, lambda gt: gt * deep, 1, 3)
    prv = first(3, lambda gt: gt * deep + deep - 1, 3, 1)
    own_up = first(0, lambda gt: lax.rem(z + 1, lines), 0, 0)
    own_dn = first(0, lambda gt: lax.rem(z + lines - 1, lines), 4, 0)

    def each(copies, what):
        def run_all():
            for copy in copies:
                getattr(copy, what)()

        return run_all

    wd_copy = remote(wd_hbm.at[:, :, peer_cols], wd.at[core], wd_send.at[0], wd_recv.at[0], other_core)
    wd_copy.start()
    zbuf[0, late, lax.rem(o, two)] = packed[grp]
    meta_in[0, o] = meta_out[grp]

    def onward(plus):
        zz = lax.rem(z + plus * 2 - 1 + lines, lines)
        more = ((plus == 1) & (o < deep - 1)) | ((plus == 0) & (o > 0))
        return zz, more

    def z_copy(d, s, plus, q):
        zz, more = onward(plus)
        here = chunk(d, s, q)
        return remote(here, here, z_send.at[d, s, q], z_recv.at[d, s, q], at_z(zz)), more

    def arrive(d, s, plus):
        for q in range(PARTS):
            copy, more = z_copy(d, s, plus, q)
            copy.wait_recv()
            pl.when(more)(copy.start)

    pair = two * gmax
    run = two * cap

    def x_to(src, dst, send, recv, d, h, j):
        xx = lax.rem(x + j, cols)
        return remote(src.at[d, h, xx], dst.at[d, h, x], send.at[d, h, j], recv.at[d, h, j], at_x(xx))

    def x_from(src, dst, send, recv, d, h, j):
        xx = lax.rem(x + cols - j, cols)
        return remote(src.at[d, h, xx], dst.at[d, h, xx], send.at[d, h, j], recv.at[d, h, j], at_x(xx))

    out_args = (xsend, rows.at[core], x_send, x_recv)
    back_args = (back_out, back_in, b_send, b_recv)
    x_order = [1, cols - 1] + list(range(2, cols - 1))

    def d_copy(d, h):
        return remote(rows.at[core, d, h], rows.at[core, d, h], d_send.at[d, h], d_recv.at[d, h], other_core)

    def d_arrival(d, h):
        return remote(rows.at[peer, d, h], rows.at[peer, d, h], d_send.at[d, h], d_recv.at[d, h], other_core)

    def select(d, h):
        for i in range(two):
            s = two * h + i
            pl.when((d != 0) | (s != o))(
                remote(meta_out.at[0], meta_in.at[d, s], m_send.at[0], m_recv.at[d, s], at_z(z)).wait_recv
            )
        lane = iota((2 * top, 2 * gmax), 1)
        info = jnp.where(lane < gmax, meta_in[d, two * h], meta_in[d, two * h + 1])
        zs = lax.div(iota((1, pair), 1), gmax)
        s_io = iota((pair, pair), 0)
        a = jnp.zeros((pair, pair), F32)
        w = jnp.zeros((pair, pair), F32)
        span = cols * loc * cap
        for k in range(top):
            v = info[k : k + 1, :].astype(I32) - 1 - span * o
            ok = (v >= 0) & (v < span)
            sid = jnp.where(ok, lax.div(v, cap) * run + zs * cap + lax.rem(v, cap), -1)
            hit = s_io == sid
            a = jnp.where(hit, 1.0, a)
            w = jnp.where(hit, info[top + k : top + k + 1, :], w)
        picked = mm(a.astype(BF16), zbuf[d, h].reshape(pair, half)).astype(BF16)
        xsend[d, h] = picked.reshape(cols, loc * run, half)
        for j in x_order:
            x_to(*out_args, d, h, j).start()
        rows[core, d, h, x] = xsend[d, h, x]
        hi = w.astype(BF16)
        mix_hi[d, h] = hi
        mix_lo[d, h] = (w - hi.astype(F32)).astype(BF16)

    def exchange(d, h):
        for j in x_order:
            x_from(*out_args, d, h, j).wait_recv()
        d_copy(d, h).start()

    m = cols * run

    def h_copy(d, h):
        return remote(hid.at[core, d, h], hid.at[core, d, h], h_send.at[d, h], h_recv.at[d, h], other_core)

    def h_arrival(d, h):
        return remote(hid.at[peer, d, h], hid.at[peer, d, h], h_send.at[d, h], h_recv.at[d, h], other_core)

    def gate_up(d, h):
        d_arrival(d, h).wait_recv()
        for e in range(loc):
            r = [rows[c, d, h, :, e * run : (e + 1) * run, :].reshape(m, half) for c in range(2)]
            ga = mm(r[0], wg[e, :half, :]) + mm(r[1], wg[e, half:, :])
            up = mm(r[0], wu[e, :half, :]) + mm(r[1], wu[e, half:, :])
            hid[core, d, h, e] = (ga / (1.0 + jnp.exp(-ga)) * up).astype(BF16)
        h_copy(d, h).start()

    def down(d, h):
        h_arrival(d, h).wait_recv()
        for e in range(loc):
            y = mm(hid[0, d, h, e], wd[0, e]) + mm(hid[1, d, h, e], wd[1, e])
            back_out[d, h, :, e * run : (e + 1) * run, :] = y.astype(BF16).reshape(cols, run, half)
        for j in x_order:
            x_to(*back_args, d, h, j).start()
        back_in[d, h, x] = back_out[d, h, x]

    def combine(d, h):
        for j in x_order:
            x_from(*back_args, d, h, j).wait_recv()
        res = back_in[d, h].reshape(pair, half)
        part[d, h] = mm_tn(mix_hi[d, h], res) + mm_tn(mix_lo[d, h], res)

    def landing(d, s, q, at, zz):
        return remote(
            psend.at[d, s, bits[q]], land.at[at, bits[q]], p_send.at[d, s, q], l_recv.at[at, q], at_z(zz)
        )

    def mine(d, s, q):
        at = pl.multiple_of(lax.rem(s, two) * gmax + q * bit, bit)
        return part[d, lax.div(s, two), pl.ds(at, bit), :]

    def send_back(d, s, plus):
        _, more = onward(plus)
        own = (d == 0).astype(I32)
        home = (1 - own) * (o == (deep - 1) * (1 - plus)).astype(I32)
        near = own * (s + plus * 2 - 1 == o).astype(I32)
        chain = d * deep + s
        at = home * (home_at + grp) + near * (side_at + 1 - plus) + (1 - home - near) * chain
        beside = lax.rem(z - (plus * 2 - 1) + lines, lines)
        zz = home * (lax.rem(grp + d, GROUPS) * deep + s) + (1 - home) * beside
        for q in range(PARTS):

            @pl.when(more)
            def _():
                landing(d, s, q, chain, z).wait_recv()
                psend[d, s, bits[q]] = (mine(d, s, q) + land[chain, bits[q]].astype(F32)).astype(BF16)

            @pl.when(jnp.logical_not(more))
            def _():
                psend[d, s, bits[q]] = mine(d, s, q).astype(BF16)

            landing(d, s, q, at, zz).start()

    def mirrored(kind, d, s):
        return (GROUPS - d) % GROUPS, (deep if kind in (ARRIVE, BACK) else 2) - 1 - s

    def pick(values):
        if len(set(values)) == 1:
            return jnp.int32(values[0])
        return sum(i * v for i, v in zip(in_row, values))

    def way(d, s, r):
        return {3: 1, 1: 0, 2: int(s >= two), 0: int(s < r)}[d]

    for n, (kind, d0, s0, d1, s1) in enumerate(PLAN):
        if kind == METAS:
            each(far_metas, "start")()
            continue
        if kind == WAIT_W:
            for copy in w_copies:
                copy.wait()
            remote(
                wd_hbm.at[:, :, my_cols], wd.at[peer], wd_send.at[0], wd_recv.at[0], other_core
            ).wait_recv()
            continue
        per_row = [(d0, s0), (d1, s1)]
        per_row += [mirrored(kind, *p) for p in per_row[::-1]]
        if kind == SEND:
            for t, copies in ((1, nxt), (2, opp), (3, prv)):
                flags = [int(p[0] == t) for p in per_row]
                if all(flags):
                    each(copies, "start")()
                elif any(flags):
                    pl.when(pick(flags) == 1)(each(copies, "start"))
            flags = [int(p[0] == 0) for p in per_row]
            if any(flags):
                pl.when((pick(flags) == 1) & (o < deep - 1))(each(own_up, "start"))
                pl.when((pick(flags) == 1) & (o > 0))(each(own_dn, "start"))
            continue
        d, s = pick([p[0] for p in per_row]), pick([p[1] for p in per_row])
        if kind in (ARRIVE, BACK):
            plus = pick([way(*p, r) for r, p in enumerate(per_row)])
            (arrive if kind == ARRIVE else send_back)(d, s, plus)
        else:
            {SELECT: select, EXCHANGE: exchange, GATE_UP: gate_up, DOWN: down, COMBINE: combine}[kind](d, s)

    own = jnp.concatenate([mine(0, o, q) for q in range(PARTS)], axis=0)

    @pl.when(o < deep - 1)
    def _():
        for q in range(PARTS):
            landing(0, o, q, side_at, z).wait_recv()

    @pl.when(o > 0)
    def _():
        for q in range(PARTS):
            landing(0, o, q, side_at + 1, z).wait_recv()

    own = own + jnp.where(o < deep - 1, land[side_at].astype(F32), 0.0)
    own = own + jnp.where(o > 0, land[side_at + 1].astype(F32), 0.0)
    for t in (1, 3, 2):
        gt = lax.rem(grp + t, GROUPS)
        for q in range(PARTS):
            landing(0, o, q, home_at + gt, z).wait_recv()
    land[home_at + grp] = own.astype(BF16)
    returned = land[home_at : home_at + GROUPS].reshape(GROUPS * gmax, half)
    mixed = mm_tn(place[...], returned)
    sq = jnp.zeros((tok, 128), F32)
    for i in range(half // 128):
        v = mixed[:, i * 128 : (i + 1) * 128]
        sq = sq + v * v
    sq_out[...] = sq
    q_copy = remote(sq_out, sq_in, q_send.at[0], q_recv.at[0], other_core)
    q_copy.start()
    q_copy.wait_recv()
    total = jnp.sum(sq_out[...] + sq_in[...], axis=1, keepdims=True)
    out_ref[...] = (mixed * lax.rsqrt(total / width + EPS) * out_gain[...]).astype(BF16)

    q_copy.wait_send()
    each(near_metas + far_metas, "wait_send")()
    each(opp + nxt + prv, "wait_send")()
    pl.when(o < deep - 1)(each(own_up, "wait_send"))
    pl.when(o > 0)(each(own_dn, "wait_send"))
    wd_copy.wait_send()

    def sent(d, s, plus):
        copies, more = [z_copy(d, s, plus, q)[0] for q in range(PARTS)], onward(plus)[1]
        pl.when(more)(each(copies, "wait_send"))
        for q in range(PARTS):
            landing(d, s, q, 0, z).wait_send()

    for s in range(deep):
        sent(2, s, s // two)
        sent(3, s, 1)
        sent(1, s, 0)
    for j in range(1, deep):
        s = lax.rem(o + j, deep)
        sent(0, s, (s < o).astype(I32))
    for d in range(GROUPS):
        for h in range(2):
            h_copy(d, h).wait_send()
            d_copy(d, h).wait_send()
            for j in range(1, cols):
                x_to(*out_args, d, h, j).wait_send()
                x_to(*back_args, d, h, j).wait_send()


def body(tokens, in_gain, routing, gate_prob, w_gate, w_up, w_down, out_gain):
    ep_count = lax.axis_size("ep")
    loc, width, ff = w_gate.shape
    tok, top = routing.shape
    half = out_gain.shape[0]
    epg = loc * ep_count // GROUPS
    cap = max(2, tok * top // (2 * epg))
    gmax = epg * cap // top
    side = math.isqrt(ep_count // GROUPS)
    lines = ep_count // side
    cols, deep = side, side
    two = deep // 2
    pair = two * gmax
    piece = loc * two * cap
    m = cols * two * cap
    cfg = (lines, side, tok, top, cap, gmax, half, width, epg)
    vmem = pl.BlockSpec(memory_space=pltpu.VMEM)
    anyw = pl.BlockSpec(memory_space=pl.ANY)
    dma = pltpu.SemaphoreType.DMA
    scratch = [
        pltpu.VMEM(w_gate.shape, BF16),
        pltpu.VMEM(w_up.shape, BF16),
        pltpu.VMEM((2, loc, ff, half), BF16),
        pltpu.VMEM((GROUPS * gmax, tok), BF16),
        pltpu.VMEM((GROUPS, 2 * top, 2 * gmax), F32),
        pltpu.VMEM((GROUPS, deep, 2 * top, 2 * gmax), F32),
        pltpu.VMEM((GROUPS, gmax, half), BF16),
        pltpu.VMEM((GROUPS, 2, two, gmax, half), BF16),
        pltpu.VMEM((GROUPS, 2, pair, pair), BF16),
        pltpu.VMEM((GROUPS, 2, pair, pair), BF16),
        pltpu.VMEM((GROUPS, 2, cols, piece, half), BF16),
        pltpu.VMEM((2, GROUPS, 2, cols, piece, half), BF16),
        pltpu.VMEM((2, GROUPS, 2, loc, m, ff), BF16),
        pltpu.VMEM((GROUPS, 2, cols, piece, half), BF16),
        pltpu.VMEM((GROUPS, 2, cols, piece, half), BF16),
        pltpu.VMEM((GROUPS, 2, pair, half), F32),
        pltpu.VMEM((GROUPS, deep, gmax, half), BF16),
        pltpu.VMEM((GROUPS * deep + GROUPS + 2, gmax, half), BF16),
        pltpu.VMEM((tok, 128), F32),
        pltpu.VMEM((tok, 128), F32),
        dma((3,)),
        dma((1,)),
        dma((1,)),
        dma((lines,)),
        dma((GROUPS, deep)),
        dma((5, PARTS)),
        dma((GROUPS, deep, PARTS)),
        dma((GROUPS, deep, PARTS)),
        dma((GROUPS, 2, cols)),
        dma((GROUPS, 2, cols)),
        dma((GROUPS, 2)),
        dma((GROUPS, 2)),
        dma((GROUPS, 2)),
        dma((GROUPS, 2)),
        dma((GROUPS, 2, cols)),
        dma((GROUPS, 2, cols)),
        dma((GROUPS, deep, PARTS)),
        dma((GROUPS * deep + GROUPS + 2, PARTS)),
        dma((1,)),
        dma((1,)),
    ]
    return pl.pallas_call(
        functools.partial(kernel, cfg),
        out_shape=jax.ShapeDtypeStruct((tok, half), BF16),
        in_specs=[vmem] * 5 + [anyw] * 3,
        out_specs=vmem,
        scratch_shapes=scratch,
        compiler_params=pltpu.CompilerParams(
            collective_id=0, has_side_effects=True, vmem_limit_bytes=60 * 1024 * 1024
        ),
    )(
        routing.T, gate_prob.T, tokens, in_gain.reshape(1, width), out_gain.reshape(1, half),
        w_gate, w_up, w_down,
    )


def solution(mesh):
    placed = (
        P(("grp", "ep"), None),
        P(),
        P(("grp", "ep"), None),
        P(("grp", "ep"), None),
        P("ep", None, "tp"),
        P("ep", None, "tp"),
        P("ep", "tp", None),
        P("tp"),
    )
    return jax.shard_map(
        body, mesh=mesh, in_specs=placed, out_specs=P(("grp", "ep"), "tp"), check_vma=False
    )
```
